32 devices in a mesh: grp: 2 (over x), ep: 16 (over z, y, core).
Axes of the slice: x: 2, y: 2, z: 4, core: 2. Of those that a mesh axis runs over, the one named last changes fastest.
Arguments:
- tokens: bfloat16 [256, 2048], P(('grp', 'ep')), parts along dimension 0, may hold values from -6 to 6
- first_gain: bfloat16 [2048], replicated, may hold values from 0.099609375 to 1.8984375
- query_weight: bfloat16 [2048, 1024], P(None, 'ep'), may hold values from -0.125 to 0.125
- key_weight: bfloat16 [2048, 1024], P(None, 'ep'), may hold values from -0.125 to 0.125
- value_weight: bfloat16 [2048, 1024], P(None, 'ep'), may hold values from -0.125 to 0.125
- outgate_weight: bfloat16 [2048, 1024], P(None, 'ep'), may hold values from -0.125 to 0.125
- igate_weight: bfloat16 [2048, 8], replicated, may hold values from -0.125 to 0.125
- fgate_weight: bfloat16 [2048, 8], replicated, may hold values from -0.125 to 0.125
- igate_bias: float32 [8], replicated, may hold values from -2 to 1
- fgate_bias: float32 [8], replicated, may hold values from -1 to 4
- memory_state: float32 [256, 8, 128, 128], P(('grp', 'ep')), parts along dimension 0, may hold values from -0.6 to 0.6
- norm_state: float32 [256, 8, 128], P(('grp', 'ep')), parts along dimension 0, may hold values from -0.6 to 0.6
- max_state: float32 [256, 8], P(('grp', 'ep')), parts along dimension 0, may hold values from -1 to 2
- head_gain: bfloat16 [1024], replicated, may hold values from 0.099609375 to 1.8984375
- out_weight: bfloat16 [1024, 2048], P('ep'), may hold values from -0.1875 to 0.1875
- second_gain: bfloat16 [2048], replicated, may hold values from 0.099609375 to 1.8984375
- expert_ids: int32 [256, 6], P(('grp', 'ep')), parts along dimension 0, may hold values from 0 to 15, all different within a row; in each aligned block of 8 rows (0 to 7, 8 to 15, ...) at most 6 rows name the same one
- route_weight: float32 [256, 6], P(('grp', 'ep')), parts along dimension 0, may hold values from 0.2 to 1
- expert_gate: bfloat16 [16, 2048, 256], P('ep'), may hold values from -0.125 to 0.125
- expert_up: bfloat16 [16, 2048, 256], P('ep'), may hold values from -0.125 to 0.125
- expert_down: bfloat16 [16, 256, 2048], P('ep'), may hold values from -0.375 to 0.375
- shared_gate: bfloat16 [2048, 256], P('ep'), may hold values from -0.125 to 0.125
- shared_up: bfloat16 [2048, 256], P('ep'), may hold values from -0.125 to 0.125
- shared_down: bfloat16 [256, 2048], P(None, 'ep'), may hold values from -0.375 to 0.375
Outputs:
- mixed_out: bfloat16 [256, 2048], P(('grp', 'ep')), parts along dimension 0
- memory_next: float32 [256, 8, 128, 128], P(('grp', 'ep')), parts along dimension 0
- norm_next: float32 [256, 8, 128], P(('grp', 'ep')), parts along dimension 0
- max_next: float32 [256, 8], P(('grp', 'ep')), parts along dimension 0
The draws below stay inside these ranges and needn't reach their ends.
There are 2 independent parts, one for each index of `grp`. The reference program is written for one: setup_inputs(seed, part) draws one part's arguments, and reference() takes and returns one part's arrays. A program takes and returns all parts, laid end to end along the dimension named above; an argument that names none is the same for every part. Nothing has to cross between parts.
Inputs may be any that keep to these rules, and one draw needn't show every extreme that they name: `expert_ids`: each row names 6 different experts. Among the rows of one device no expert is named by more than 6 rows, and in every draw some expert is named by exactly 6 rows of some device.
All inputs are finite; a program needn't handle non-finite values.
Results may differ from the reference program's by a relative error of at most 0.013.
Values may be sent and summed in bfloat16 or wider, within the bound.
A program may use at most 64 MiB of HBM per device.

```python
import math
import jax
import jax.numpy as jnp
import numpy as np
from jax import lax

D = 2048
HEADS = 8
DK = 128
FE = 256
FS = 256
TOP_K = 6
SEQ_DEV = 8
MW = 1024
SEQS = 128
EXPERTS = 16
CAP = 6
N_EP = 16


def levels(own_key, shape, pieces, low, high):
    loudness, own = 1.0, jax.random.fold_in(own_key, 6)
    for axis_at, parts in pieces:
        draws = jnp.exp(jax.random.uniform(jax.random.fold_in(own, axis_at), (parts,), jnp.float32, low / len(pieces), high / len(pieces)))
        loudness = loudness * jnp.repeat(draws, shape[axis_at] // parts).reshape([-1 if axis == axis_at else 1 for axis in range(len(shape))])
    return loudness


def routed_block(key, own, number, rows, number_of, top, reach, slope):
    sequence = jax.random.permutation(key, number_of)
    crowded, usual = portions_of(number_of, rows * top, reach, slope, True), portions_of(number_of, rows * top, reach, slope, False)
    places = jnp.arange(number_of)

    def named(tallies, turn):
        used = int((tallies > 0).sum())
        fixed = max(1, used // 4)
        shifted = fixed + (places - fixed + turn * (used - fixed)) % max(1, number_of - fixed)
        return jnp.zeros((number_of,), jnp.int32).at[sequence[jnp.where(places < fixed, places, shifted)]].set(jnp.asarray(tallies, jnp.int32))

    tallies = jnp.where(number % 4 == 0, named(crowded, number // 4), named(usual, number - number // 4 - 1))
    mixed = jax.random.permutation(jax.random.fold_in(own, 3), number_of)
    giver, sink = mixed[0:number_of // 2 * 2:2], mixed[1:number_of // 2 * 2:2]
    room = jnp.minimum(tallies[giver] - 1, reach - tallies[sink]) // 2
    room = jnp.where((giver == sequence[0]) | (sink == sequence[0]) | (tallies[sink] == 0), 0, jnp.maximum(room, 0))
    shifted = jax.random.randint(jax.random.fold_in(own, 4), (number_of // 2,), 0, 1 << 20) % (room + 1)
    tallies = tallies.at[giver].add(-shifted).at[sink].add(shifted)
    items = jnp.searchsorted(jnp.cumsum(tallies), jnp.arange(rows * top), side="right").astype(jnp.int32)
    listing = items.reshape(top, rows).T
    listing = listing[jax.random.permutation(jax.random.fold_in(own, 1), rows)]
    turn = jax.random.randint(jax.random.fold_in(own, 2), (rows, 1), 0, top)
    return jnp.take_along_axis(listing, (jnp.arange(top)[None, :] + turn) % top, axis=1)


def portions_of(number_of, total, limit, slope, full):
    portions = [(1 << 20) // math.isqrt(rank ** slope) + 1 for rank in range(1, number_of + 1)]
    largest = limit if full else min(limit, max(-(-total // number_of), total * portions[0] // sum(portions)))
    least = 1 if total - largest >= number_of - 1 else 0
    given, rest = [largest] + [least] * (number_of - 1), total - largest - least * (number_of - 1)
    while rest > 0:
        candidates = [i for i in range(1, number_of) if given[i] < largest] or [i for i in range(1, number_of) if given[i] < limit]
        mass, budget = sum([portions[i] for i in candidates]), rest
        for i in candidates:
            addition = min(limit - given[i], max(1, budget * portions[i] // mass), rest)
            given[i] = given[i] + addition
            rest = rest - addition
    return np.array(given)


def noise(key, shape, spread, limit, split=(), kind=jnp.bfloat16):
    loudness = levels(key, shape, split, -0.22, 0.18) if split else 1.0
    drawn = jax.random.normal(key, shape, jnp.float32) * spread * loudness
    return jnp.minimum(jnp.maximum(drawn, -limit), limit).astype(kind)


def setup_inputs(seed: int = 0, part: int = 0) -> dict:
    arg_keys = jax.random.split(jax.random.key(seed), 25)
    own_keys = jax.random.split(jax.random.fold_in(arg_keys[24], part), 25)
    tokens = noise(own_keys[0], (SEQS, D), 1.0, 6.0, ((0, 16),))
    first_gain = jnp.clip(1.0 + 0.18 * jax.random.normal(arg_keys[1], (D,), jnp.float32), 0.099609375, 1.8984375).astype(jnp.bfloat16)
    query_weight = noise(arg_keys[2], (D, MW), D ** -0.5, 0.125, ((1, 16),))
    key_weight = noise(arg_keys[3], (D, MW), D ** -0.5, 0.125, ((1, 16),))
    value_weight = noise(arg_keys[4], (D, MW), D ** -0.5, 0.125, ((1, 16),))
    outgate_weight = noise(arg_keys[5], (D, MW), D ** -0.5, 0.125, ((1, 16),))
    igate_weight = noise(arg_keys[6], (D, HEADS), D ** -0.5, 0.125)
    fgate_weight = noise(arg_keys[7], (D, HEADS), D ** -0.5, 0.125)
    igate_bias = jnp.clip(jax.random.uniform(arg_keys[8], (HEADS,), jnp.float32, -2.0, 1.0), -2.0, 1.0)
    fgate_bias = jnp.clip(jax.random.uniform(arg_keys[9], (HEADS,), jnp.float32, -1.0, 4.0), -1.0, 4.0)
    memory_state = noise(own_keys[10], (SEQS, HEADS, DK, DK), 0.1, 0.6, ((0, 16),), jnp.float32)
    norm_state = noise(own_keys[11], (SEQS, HEADS, DK), 0.1, 0.6, ((0, 16),), jnp.float32)
    max_state = jnp.clip(-1.0 + 3.0 * jax.random.uniform(own_keys[12], (SEQS, HEADS), jnp.float32) ** levels(own_keys[12], (SEQS, HEADS), ((0, 16),), -0.2, 0.2), -1.0, 2.0)
    head_gain = jnp.clip(1.0 + 0.18 * jax.random.normal(arg_keys[13], (MW,), jnp.float32), 0.099609375, 1.8984375).astype(jnp.bfloat16)
    out_weight = noise(arg_keys[14], (MW, D), MW ** -0.5, 0.1875, ((0, 16),))
    second_gain = jnp.clip(1.0 + 0.18 * jax.random.normal(arg_keys[15], (D,), jnp.float32), 0.099609375, 1.8984375).astype(jnp.bfloat16)
    expert_ids_keys = jax.random.split(jax.random.fold_in(own_keys[16], 1), SEQS // SEQ_DEV)
    expert_ids_turns = jax.random.permutation(jax.random.fold_in(own_keys[16], 3), SEQS // SEQ_DEV)
    expert_ids = jax.vmap(lambda own, number: routed_block(jax.random.fold_in(own_keys[16], 2), own, number, SEQ_DEV, EXPERTS, TOP_K, CAP, 1))(expert_ids_keys, expert_ids_turns).reshape((SEQS, TOP_K))
    route_weight = jnp.clip(0.2 + 0.8 * jax.random.uniform(own_keys[17], (SEQS, TOP_K), jnp.float32) ** levels(own_keys[17], (SEQS, TOP_K), ((0, 16),), -0.2, 0.2), 0.2, 1.0)
    expert_gate = noise(arg_keys[18], (EXPERTS, D, FE), D ** -0.5, 0.125, ((0, 16),))
    expert_up = noise(arg_keys[19], (EXPERTS, D, FE), D ** -0.5, 0.125, ((0, 16),))
    expert_down = noise(arg_keys[20], (EXPERTS, FE, D), FE ** -0.5, 0.375, ((0, 16),))
    shared_gate = noise(arg_keys[21], (D, FS), D ** -0.5, 0.125, ((0, 16),))
    shared_up = noise(arg_keys[22], (D, FS), D ** -0.5, 0.125, ((0, 16),))
    shared_down = noise(arg_keys[23], (FS, D), FS ** -0.5, 0.375, ((1, 16),))
    return dict(tokens=tokens, first_gain=first_gain, query_weight=query_weight, key_weight=key_weight, value_weight=value_weight, outgate_weight=outgate_weight, igate_weight=igate_weight, fgate_weight=fgate_weight, igate_bias=igate_bias, fgate_bias=fgate_bias, memory_state=memory_state, norm_state=norm_state, max_state=max_state, head_gain=head_gain, out_weight=out_weight, second_gain=second_gain, expert_ids=expert_ids, route_weight=route_weight, expert_gate=expert_gate, expert_up=expert_up, expert_down=expert_down, shared_gate=shared_gate, shared_up=shared_up, shared_down=shared_down)


epsilon = 1e-06

def rms_scale(values, gain):
    return values * lax.rsqrt(lax.optimization_barrier(jnp.mean(values * values, axis=-1, keepdims=True)) + epsilon) * gain.astype(jnp.float32)

def cell_step(normed, query, key_proj, value_proj, outgate, igate_weight, fgate_weight, igate_bias, fgate_bias, memory_state, norm_state, max_state, head_gain):
    row_count, head_count = max_state.shape
    head_size = memory_state.shape[-1]
    input_gate = jnp.dot(normed, igate_weight, preferred_element_type=jnp.float32) + igate_bias
    forget_log = jax.nn.log_sigmoid(jnp.dot(normed, fgate_weight, preferred_element_type=jnp.float32) + fgate_bias)
    query_heads = query.astype(jnp.float32).reshape(row_count, head_count, head_size)
    key_heads = key_proj.astype(jnp.float32).reshape(row_count, head_count, head_size) * head_size ** (-0.5)
    value_heads = value_proj.astype(jnp.float32).reshape(row_count, head_count, head_size)
    max_next = jnp.maximum(forget_log + max_state, input_gate)
    decay_rate = jnp.exp(forget_log + max_state - max_next)
    injected = jnp.exp(input_gate - max_next)
    memory_next = decay_rate[:, :, None, None] * memory_state + injected[:, :, None, None] * (key_heads[:, :, :, None] * value_heads[:, :, None, :])
    norm_next = decay_rate[:, :, None] * norm_state + injected[:, :, None] * key_heads
    numerator = jnp.einsum('shd,shde->she', query_heads, memory_next, precision=lax.Precision.HIGHEST)
    denominator = jnp.maximum(jnp.abs(lax.optimization_barrier(jnp.sum(query_heads * norm_next, axis=-1))), jnp.exp(-max_next))
    readout = numerator / denominator[:, :, None]
    readout = rms_scale(readout, head_gain.reshape(head_count, head_size))
    gated = readout.reshape(row_count, head_count * head_size) * jax.nn.sigmoid(outgate.astype(jnp.float32))
    return (gated.astype(jnp.bfloat16), memory_next, norm_next, max_next)

def expert_apply(picked_rows, gate_matrix, up_matrix, down_matrix):
    gate_sums = jnp.dot(picked_rows, gate_matrix, preferred_element_type=jnp.float32)
    up_sums = jnp.dot(picked_rows, up_matrix, preferred_element_type=jnp.float32)
    hidden = (jax.nn.silu(gate_sums) * up_sums).astype(jnp.bfloat16)
    return jnp.dot(hidden, down_matrix, preferred_element_type=jnp.float32).astype(jnp.bfloat16)

def reference(tokens, first_gain, query_weight, key_weight, value_weight, outgate_weight, igate_weight, fgate_weight, igate_bias, fgate_bias, memory_state, norm_state, max_state, head_gain, out_weight, second_gain, expert_ids, route_weight, expert_gate, expert_up, expert_down, shared_gate, shared_up, shared_down):
    inputs = tokens.astype(jnp.float32)
    normed = rms_scale(inputs, first_gain).astype(jnp.bfloat16)
    query = jnp.dot(normed, query_weight, preferred_element_type=jnp.float32).astype(jnp.bfloat16)
    key_proj = jnp.dot(normed, key_weight, preferred_element_type=jnp.float32).astype(jnp.bfloat16)
    value_proj = jnp.dot(normed, value_weight, preferred_element_type=jnp.float32).astype(jnp.bfloat16)
    outgate = jnp.dot(normed, outgate_weight, preferred_element_type=jnp.float32).astype(jnp.bfloat16)
    gated, memory_next, norm_next, max_next = cell_step(normed, query, key_proj, value_proj, outgate, igate_weight, fgate_weight, igate_bias, fgate_bias, memory_state, norm_state, max_state, head_gain)
    mix = jnp.dot(gated, out_weight, preferred_element_type=jnp.float32).astype(jnp.bfloat16)
    stream = inputs + mix.astype(jnp.float32)
    normed_two = rms_scale(stream, second_gain).astype(jnp.bfloat16)
    padded = jnp.concatenate([normed_two, jnp.zeros((1, D), normed_two.dtype)], axis=0)

    def per_expert(routed, inputs_expert):
        expert_index, gate_matrix, up_matrix, down_matrix = inputs_expert
        chosen = expert_ids == expert_index
        weight = lax.optimization_barrier(jnp.sum(jnp.where(chosen, route_weight, jnp.zeros_like(route_weight)), axis=1))
        weight_pad = jnp.concatenate([weight, jnp.zeros((1,), weight.dtype)], axis=0)
        picked = jnp.nonzero(jnp.any(chosen, axis=1), size=N_EP * CAP, fill_value=SEQS)[0].astype(jnp.int32)
        result = expert_apply(padded[picked], gate_matrix, up_matrix, down_matrix)
        routed = routed.at[picked].add(weight_pad[picked][:, None] * result.astype(routed.dtype), mode='drop')
        return (routed, None)
    routed, _ = lax.scan(per_expert, jnp.zeros((SEQS, D), jnp.float32), (jnp.arange(EXPERTS, dtype=jnp.int32), expert_gate, expert_up, expert_down))
    gate_shared = jnp.dot(normed_two, shared_gate, preferred_element_type=jnp.float32)
    up_shared = jnp.dot(normed_two, shared_up, preferred_element_type=jnp.float32)
    hidden_shared = (jax.nn.silu(gate_shared) * up_shared).astype(jnp.bfloat16)
    shared_result = jnp.dot(hidden_shared, shared_down, preferred_element_type=jnp.float32)
    mixed_out = (stream + routed + shared_result).astype(jnp.bfloat16)
    return (mixed_out, memory_next, norm_next, max_next)
```

```python
import jax
import jax.numpy as jnp
from jax import lax
from jax.experimental import pallas as pl
from jax.experimental.pallas import tpu as pltpu
from jax.sharding import PartitionSpec as P
import functools

epsilon = 1e-06


def rms_scale(values, gain):
    return (
        values
        * lax.rsqrt(jnp.mean(values * values, axis=-1, keepdims=True) + epsilon)
        * gain.astype(jnp.float32)
    )


def cell_step(
    normed,
    query,
    key_proj,
    value_proj,
    outgate,
    igate_weight,
    fgate_weight,
    igate_bias,
    fgate_bias,
    memory_state,
    norm_state,
    max_state,
    head_gain,
):
    row_count, head_count = max_state.shape
    head_size = memory_state.shape[-1]
    input_gate = jnp.dot(normed, igate_weight, preferred_element_type=jnp.float32) + igate_bias
    forget_log = jax.nn.log_sigmoid(
        jnp.dot(normed, fgate_weight, preferred_element_type=jnp.float32) + fgate_bias
    )
    query_heads = query.astype(jnp.float32).reshape(row_count, head_count, head_size)
    key_heads = key_proj.astype(jnp.float32).reshape(
        row_count, head_count, head_size
    ) * head_size ** (-0.5)
    value_heads = value_proj.astype(jnp.float32).reshape(row_count, head_count, head_size)
    max_next = jnp.maximum(forget_log + max_state, input_gate)
    decay_rate = jnp.exp(forget_log + max_state - max_next)
    injected = jnp.exp(input_gate - max_next)
    memory_next = decay_rate[:, :, None, None] * memory_state + injected[:, :, None, None] * (
        key_heads[:, :, :, None] * value_heads[:, :, None, :]
    )
    norm_next = decay_rate[:, :, None] * norm_state + injected[:, :, None] * key_heads
    numerator = jnp.einsum(
        "shd,shde->she", query_heads, memory_next, precision=lax.Precision.HIGHEST
    )
    denominator = jnp.maximum(
        jnp.abs(jnp.sum(query_heads * norm_next, axis=-1)), jnp.exp(-max_next)
    )
    readout = numerator / denominator[:, :, None]
    readout = rms_scale(readout, head_gain.reshape(head_count, head_size))
    gated = readout.reshape(row_count, head_count * head_size) * jax.nn.sigmoid(
        outgate.astype(jnp.float32)
    )
    return (gated.astype(jnp.bfloat16), memory_next, norm_next, max_next)


def shards(
    tokens,
    first_gain,
    query_weight,
    key_weight,
    value_weight,
    outgate_weight,
    igate_weight,
    fgate_weight,
    igate_bias,
    fgate_bias,
    memory_state,
    norm_state,
    max_state,
    head_gain,
    out_weight,
    second_gain,
    expert_ids,
    route_weight,
    expert_gate,
    expert_up,
    expert_down,
    shared_gate,
    shared_up,
    shared_down,
):
    own_rows = tokens.shape[0]
    devices = lax.axis_size("ep")
    top_count = expert_ids.shape[1]
    capacity = max(2, 2 * own_rows * top_count // devices)
    inputs = tokens.astype(jnp.float32)
    normed = rms_scale(inputs, first_gain).astype(jnp.bfloat16)
    block_rows = lax.all_gather(normed, "ep", axis=0, tiled=True)
    columns = jnp.stack(
        [
            jnp.dot(block_rows, matrix, preferred_element_type=jnp.float32).astype(jnp.bfloat16)
            for matrix in (query_weight, key_weight, value_weight, outgate_weight)
        ]
    )
    projected = lax.all_to_all(columns, "ep", split_axis=1, concat_axis=2, tiled=True)
    gated, memory_next, norm_next, max_next = cell_step(
        normed,
        projected[0],
        projected[1],
        projected[2],
        projected[3],
        igate_weight,
        fgate_weight,
        igate_bias,
        fgate_bias,
        memory_state,
        norm_state,
        max_state,
        head_gain,
    )
    picked = gated
    mix_sums = jnp.dot(
        picked,
        lax.all_gather(out_weight, "ep", axis=0, tiled=True),
        preferred_element_type=jnp.float32,
    )
    stream = inputs + mix_sums.astype(jnp.bfloat16).astype(jnp.float32)
    normed_two = rms_scale(stream, second_gain).astype(jnp.bfloat16)
    block_rows = (
        lax.all_gather(shared_gate, "ep", axis=0, tiled=True),
        lax.all_gather(shared_up, "ep", axis=0, tiled=True),
    )
    picked = normed_two
    gate_shared = jnp.dot(picked, block_rows[0], preferred_element_type=jnp.float32)
    up_shared = jnp.dot(picked, block_rows[1], preferred_element_type=jnp.float32)
    hidden_shared = (jax.nn.silu(gate_shared) * up_shared).astype(jnp.bfloat16)
    shared_result = jnp.dot(
        hidden_shared,
        lax.all_gather(shared_down, "ep", axis=1, tiled=True),
        preferred_element_type=jnp.float32,
    )
    choose = (expert_ids[:, :, None] == jnp.arange(devices, dtype=jnp.int32)[None, None, :]).astype(
        jnp.int32
    )
    counted = jnp.sum(choose, axis=1)
    ranking = jnp.cumsum(counted, axis=0) - counted
    slot_index = jnp.sum(choose * ranking[:, None, :], axis=2)
    slot_ids = jnp.arange(capacity, dtype=jnp.int32)
    selector = counted.T[:, None, :] * (ranking.T[:, None, :] == slot_ids[None, :, None]).astype(
        jnp.int32
    )
    outgoing = jnp.einsum(
        "ecr,rd->ecd", selector.astype(jnp.bfloat16), normed_two, preferred_element_type=jnp.float32
    ).astype(jnp.bfloat16)
    arrived = lax.all_to_all(outgoing, "ep", split_axis=0, concat_axis=0, tiled=True)
    sources, slots, width = arrived.shape
    flat_rows = arrived.reshape(sources * slots, width)
    gate_sums = jnp.dot(flat_rows, expert_gate[0], preferred_element_type=jnp.float32)
    up_sums = jnp.dot(flat_rows, expert_up[0], preferred_element_type=jnp.float32)
    hidden = (jax.nn.silu(gate_sums) * up_sums).astype(jnp.bfloat16)
    result = jnp.dot(hidden, expert_down[0], preferred_element_type=jnp.float32).astype(
        jnp.bfloat16
    )
    results = lax.all_to_all(
        result.reshape(sources, slots, width), "ep", split_axis=0, concat_axis=0, tiled=True
    )
    flat_results = results.reshape(devices * capacity, results.shape[2])
    picked_results = flat_results[expert_ids * capacity + slot_index]
    routed = jnp.sum(route_weight[:, :, None] * picked_results.astype(jnp.float32), axis=1)
    mixed_out = (stream + routed + shared_result).astype(jnp.bfloat16)
    return (mixed_out, memory_next, norm_next, max_next)


ANY, VMEM = pl.ANY, pltpu.VMEM
F32, BF16 = jnp.float32, jnp.bfloat16


def remote(source, target, send, receive, device):
    return pltpu.make_async_remote_copy(
        src_ref=source,
        dst_ref=target,
        send_sem=send,
        recv_sem=receive,
        device_id={"ep": device},
        device_id_type=pl.DeviceIdType.MESH,
    )


def across(left, right):
    return lax.dot_general(left, right, (((1,), (1,)), ((), ())), preferred_element_type=F32)


def in_line(gain):
    held = gain[...].astype(F32)
    return jnp.concatenate([held[i : i + 1] for i in range(held.shape[0])], axis=1)


def fused(
    n,
    tokens,
    first_gain,
    query_weight,
    key_weight,
    value_weight,
    outgate_weight,
    igate_weight,
    fgate_weight,
    igate_bias,
    fgate_bias,
    memory_state,
    norm_state,
    max_state,
    head_gain,
    out_weight,
    second_gain,
    expert_ids,
    route_weight,
    expert_gate,
    expert_up,
    expert_down,
    shared_gate,
    shared_up,
    shared_down,
    mixed_out,
    memory_next,
    norm_next,
    max_next,
    proj,
    gates_in,
    memory,
    out_pad,
    wide,
    down,
    rows_one,
    rows_two,
    table,
    column_send,
    column_recv,
    shared_send,
    shared_recv,
    sdown_recv,
    gated_send,
    gated_recv,
    part,
    part_send,
    pair_recv,
    sum_send,
    sum_recv,
    local_sem,
    memory_in_sem,
    send_sem,
    recv_sem,
    gather_sem,
    pair_sem,
    sum_sem,
):
    rows, width = tokens.shape
    heads, size = memory_state.shape[1], memory_state.shape[3]
    cut = query_weight.shape[0]
    share = size // cut
    hidden = shared_gate.shape[1] // n
    top_count = expert_ids.shape[1]
    chips = n // 2
    me = lax.axis_index("ep")
    side, chip = me % 2, me // 2
    partner = me + 1 - 2 * side

    barrier = pltpu.get_barrier_semaphore()
    for k in range(1, n):
        pl.semaphore_signal(
            barrier,
            inc=1,
            device_id={"ep": (me + k) % n},
            device_id_type=pl.DeviceIdType.MESH,
        )

    loads = []

    def load(source, target):
        copy = pltpu.make_async_copy(source, target, local_sem.at[len(loads)])
        copy.start()
        loads.append(copy)
        return copy

    proj_loads = [
        load(matrix, proj.at[pl.ds(i * cut, cut)])
        for i, matrix in enumerate((query_weight, key_weight, value_weight, outgate_weight))
    ]
    gate_loads = [load(igate_weight, gates_in.at[0]), load(fgate_weight, gates_in.at[1])]
    memory_loads = []
    for h in range(heads):
        copy = pltpu.make_async_copy(
            memory_state.at[:, h], memory.at[:, h], memory_in_sem.at[h]
        )
        copy.start()
        memory_loads.append(copy)
    spot = pl.multiple_of((me % share) * cut, cut)
    out_load = load(out_weight, out_pad.at[pl.ds(spot, cut)])
    wide_loads = [load(expert_gate.at[0], wide.at[0]), load(expert_up.at[0], wide.at[1])]
    down_load = load(expert_down.at[0], down)

    inputs = tokens[...].astype(F32)
    rows_one[me] = rms_scale(inputs, in_line(first_gain)).astype(BF16)

    pl.semaphore_wait(barrier, n - 1)

    def gather(buffer, which):
        sends = []
        for k in range(chips - 1, 0, -1):
            there = 2 * ((chip + k) % chips) + side
            sends.append(
                remote(
                    buffer.at[me],
                    buffer.at[me],
                    gather_sem.at[which, 0, k],
                    gather_sem.at[which, 1, k],
                    there,
                )
            )
            sends[-1].start()
        near = remote(
            buffer.at[me],
            buffer.at[me],
            gather_sem.at[which, 2, 0],
            gather_sem.at[which, 3, 0],
            partner,
        )
        near.start()
        return sends, near

    def gather_end(buffer, which, sends, near):
        passed = [near]
        for k in ORDER(chips):
            slot = 2 * ((chip + chips - k) % chips) + side
            sends[chips - 1 - k].wait_recv()
            onward = remote(
                buffer.at[slot],
                buffer.at[slot],
                gather_sem.at[which, 2, k],
                gather_sem.at[which, 3, k],
                partner,
            )
            onward.start()
            passed.append(onward)
        for copy in passed:
            copy.wait_recv()
        return sends + passed

    unsent = []
    first = gather(rows_one, 0)

    for i in range(1, share):
        other = pl.multiple_of(((me + i) % share) * cut, cut)
        out_pad[pl.ds(other, cut), :] = jnp.zeros((cut, width), BF16)
    lanes = lax.broadcasted_iota(jnp.int32, (rows, 128), 1)
    routes = jnp.zeros((rows, 128), F32)
    for t in range(top_count):
        routes = routes + jnp.where(
            expert_ids[:, t : t + 1] == lanes, route_weight[:, t : t + 1], 0.0
        )
    table[me] = routes
    for i, matrix in enumerate((shared_gate, shared_up)):
        turned = matrix[...].astype(F32).T.reshape(n, hidden, matrix.shape[0])
        shared_send[:, i * hidden : (i + 1) * hidden, :] = turned.astype(BF16)
    for copy in gate_loads:
        copy.wait()
    own = rows_one[me]
    input_gate = across(own, gates_in[0]) + igate_bias[...]
    forget_log = jax.nn.log_sigmoid(across(own, gates_in[1]) + fgate_bias[...])
    kept = forget_log + max_state[...]
    top = jnp.maximum(kept, input_gate)
    max_next[...] = top
    decay_rate = jnp.exp(kept - top)
    injected = jnp.exp(input_gate - top)
    floor = jnp.exp(-top)

    unsent += gather_end(rows_one, 0, *first)

    def flat(buffer):
        held = buffer[...].astype(F32)
        return held.reshape(n * rows, held.shape[2])

    for copy in proj_loads:
        copy.wait()
    columns = across(flat(rows_one).astype(BF16), proj[...])
    column_send[...] = columns.reshape(n, rows, 4 * cut).astype(BF16)

    def spread(which, source, target):
        for k in range(1, n):
            there = (me + k) % n
            copy = remote(
                source(there), target, send_sem.at[which, k], recv_sem.at[which, k], there
            )
            copy.start()
            unsent.append(copy)

    def arrive(which, source, target):
        for k in range(1, n):
            remote(
                source(me), target, send_sem.at[which, k], recv_sem.at[which, k], (me + k) % n
            ).wait_recv()

    spread(0, lambda j: column_send.at[j], column_recv.at[me])
    column_recv[me] = column_send[me]
    spread(1, lambda j: table.at[me], table.at[me])
    arrive(0, lambda j: column_send.at[j], column_recv.at[me])
    spread(2, lambda j: shared_send.at[j], shared_recv.at[me])
    shared_recv[me] = shared_send[me]
    spread(3, lambda j: shared_down.at[j], sdown_recv.at[me])
    sdown_recv[me] = shared_down[me]

    place = lax.broadcasted_iota(jnp.int32, (rows, rows * size), 1) // size
    diagonal = place == lax.broadcasted_iota(jnp.int32, (rows, rows * size), 0)
    ones = jnp.where(diagonal, 1.0, 0.0)
    blocks = jnp.concatenate([ones, jnp.zeros_like(ones)], axis=0)

    def turned_dot(left, right):
        return lax.dot_general(
            left.astype(BF16),
            right.astype(BF16),
            (((0,), (0,)), ((), ())),
            preferred_element_type=F32,
        )

    for h in range(heads):
        pieces = [column_recv[h * share + i].astype(F32) for i in range(share)]
        query, keyed, valued, outgate = [
            jnp.concatenate([piece[:, i * cut : (i + 1) * cut] for piece in pieces], axis=1)
            for i in range(4)
        ]
        scale = injected[:, h : h + 1] * size ** (-0.5)
        decay = jnp.broadcast_to(decay_rate[:, h : h + 1], (rows, size))
        norm = decay * norm_state[:, h, :] + scale * keyed
        norm_next[:, h, :] = norm
        bottom = jnp.maximum(
            jnp.abs(jnp.sum(query * norm, axis=-1, keepdims=True)), floor[:, h : h + 1]
        )
        spread_value = jnp.where(diagonal, jnp.concatenate([scale * valued] * rows, axis=1), 0.0)
        high = spread_value.astype(BF16).astype(F32)
        outer = turned_dot(
            jnp.concatenate([keyed, keyed], axis=0),
            jnp.concatenate([high, spread_value - high], axis=0),
        )
        wide_query = turned_dot(jnp.concatenate([query, query * 0.0], axis=0), blocks)
        memory_loads[h].wait()
        tops = []
        for s in range(rows):
            cell = decay[s : s + 1, :] * memory[s, h] + outer[:, s * size : (s + 1) * size]
            memory_next[s, h] = cell
            tops.append(
                jnp.sum(
                    wide_query[:, s * size : (s + 1) * size] * cell, axis=0, keepdims=True
                )
            )
        readout = jnp.concatenate(tops, axis=0) / bottom
        readout = rms_scale(readout, head_gain[h : h + 1, :])
        gated_send[h] = (readout * jax.nn.sigmoid(outgate)).astype(BF16)

    spread(4, lambda j: gated_send.at[j // share], gated_recv.at[me])
    gated_recv[me] = gated_send[me // share]
    out_load.wait()
    arrive(4, lambda j: gated_send.at[j // share], gated_recv.at[me])

    def scatter(which, total, value):
        part[...] = value.reshape(n, rows, width)
        pair = []
        for k in list(range(1, chips)) + [0]:
            c = (chip + k) % chips
            part_send[which, c] = part[2 * c + 1 - side].astype(BF16)
            copy = remote(
                part_send.at[which, c],
                pair_recv.at[which, c],
                pair_sem.at[which, 0, k],
                pair_sem.at[which, 1, k],
                partner,
            )
            copy.start()
            pair.append((k, c, copy))
        sends = []
        for k, c, copy in pair:
            copy.wait_recv()
            both = part[2 * c + side] + pair_recv[which, c].astype(F32)
            if k == 0:
                total = total + both if total is not None else both
                continue
            sum_send[which, c] = both.astype(BF16)
            away = remote(
                sum_send.at[which, c],
                sum_recv.at[which, chip],
                sum_sem.at[which, 0, k],
                sum_sem.at[which, 1, k],
                2 * c + side,
            )
            away.start()
            sends.append((k, away))
        for k, away in sends:
            away.wait_recv()
            total = total + sum_recv[which, (chip + chips - k) % chips].astype(F32)
        unsent.extend([copy for _, _, copy in pair] + [away for _, away in sends])
        return total

    mix = scatter(
        0, None, jnp.dot(flat(gated_recv).astype(BF16), out_pad[...], preferred_element_type=F32)
    )
    stream = tokens[...].astype(F32) + mix.astype(BF16).astype(F32)
    rows_two[me] = rms_scale(stream, in_line(second_gain)).astype(BF16)
    second = gather(rows_two, 1)
    for copy in wide_loads + [down_load]:
        copy.wait()
    arrive(1, lambda j: table.at[me], table.at[me])
    arrive(2, lambda j: shared_send.at[j], shared_recv.at[me])
    arrive(3, lambda j: shared_down.at[j], sdown_recv.at[me])
    weights = flat(table)
    mine = lax.broadcasted_iota(jnp.int32, weights.shape, 1) == me
    weight = jnp.sum(jnp.where(mine, weights, 0.0), axis=1, keepdims=True)
    shared_wide = jnp.concatenate([shared_recv[i] for i in range(n)], axis=1)
    shared_rows = jnp.concatenate([sdown_recv[i] for i in range(n)], axis=1)
    unsent += gather_end(rows_two, 1, *second)

    block = flat(rows_two).astype(BF16)
    gate_sums = jnp.dot(block, wide[0], preferred_element_type=F32)
    up_sums = jnp.dot(block, wide[1], preferred_element_type=F32)
    own_hidden = (jax.nn.silu(gate_sums) * up_sums).astype(BF16)
    both = across(block, shared_wide)
    shared_hidden = (jax.nn.silu(both[:, :hidden]) * both[:, hidden:]).astype(BF16)
    value = weight * jnp.dot(own_hidden, down[...], preferred_element_type=F32) + jnp.dot(
        shared_hidden, shared_rows, preferred_element_type=F32
    )
    mixed_out[...] = scatter(1, stream, value).astype(BF16)

    for copy in unsent:
        copy.wait_send()


def ORDER(chips):
    return range(chips - 1, 0, -1)


def fused_shards(n, *args):
    (tokens, first_gain, query_weight, key_weight, value_weight, outgate_weight, igate_weight,
     fgate_weight, igate_bias, fgate_bias, memory_state, norm_state, max_state, head_gain,
     out_weight, second_gain, expert_ids, route_weight, expert_gate, expert_up, expert_down,
     shared_gate, shared_up, shared_down) = args
    rows, width = tokens.shape
    heads, size = memory_state.shape[1], memory_state.shape[3]
    cut = query_weight.shape[1]
    hidden = shared_gate.shape[1] // n
    chips = n // 2
    inner = expert_gate.shape[2]
    operands = (
        tokens, first_gain.reshape(-1, 128), query_weight.T, key_weight.T, value_weight.T,
        outgate_weight.T, igate_weight.T, fgate_weight.T, igate_bias.reshape(1, -1), fgate_bias.reshape(1, -1),
        memory_state, norm_state, max_state, head_gain.reshape(heads, size), out_weight,
        second_gain.reshape(-1, 128), expert_ids, route_weight, expert_gate, expert_up, expert_down,
        shared_gate, shared_up, shared_down.reshape(n, hidden, shared_down.shape[1]),
    )
    far = {2, 3, 4, 5, 6, 7, 10, 14, 18, 19, 20}
    operands = [
        pltpu.with_memory_space_constraint(x, pltpu.HBM)
        for i, x in enumerate(operands)
    ]
    dma = pltpu.SemaphoreType.DMA
    return pl.pallas_call(
        functools.partial(fused, n),
        out_shape=(
            jax.ShapeDtypeStruct((rows, width), BF16),
            jax.ShapeDtypeStruct(memory_state.shape, F32),
            jax.ShapeDtypeStruct(norm_state.shape, F32),
            jax.ShapeDtypeStruct(max_state.shape, F32),
        ),
        in_specs=[
            pl.BlockSpec(memory_space=pltpu.HBM if i in far else VMEM) for i in range(len(operands))
        ],
        out_specs=tuple(pl.BlockSpec(memory_space=m) for m in (VMEM, VMEM, VMEM, VMEM)),
        scratch_shapes=[
            VMEM((4 * cut, width), BF16),
            VMEM((2, heads, width), BF16),
            VMEM(memory_state.shape, F32),
            VMEM((size, width), BF16),
            VMEM((2, width, inner), BF16),
            VMEM((inner, width), BF16),
            VMEM((n, rows, width), BF16),
            VMEM((n, rows, width), BF16),
            VMEM((n, rows, 128), F32),
            VMEM((n, rows, 4 * cut), BF16),
            VMEM((n, rows, 4 * cut), BF16),
            VMEM((n, 2 * hidden, shared_gate.shape[0]), BF16),
            VMEM((n, 2 * hidden, shared_gate.shape[0]), BF16),
            VMEM((n, hidden, shared_down.shape[1]), BF16),
            VMEM((heads, rows, size), BF16),
            VMEM((n, rows, size), BF16),
            VMEM((n, rows, width), F32),
            VMEM((2, chips, rows, width), BF16),
            VMEM((2, chips, rows, width), BF16),
            VMEM((2, chips, rows, width), BF16),
            VMEM((2, chips, rows, width), BF16),
            dma((10,)),
            dma((heads,)),
            dma((5, n)),
            dma((5, n)),
            dma((2, 4, chips)),
            dma((2, 2, chips)),
            dma((2, 2, chips)),
        ],
        compiler_params=pltpu.CompilerParams(
            collective_id=0, has_side_effects=True, vmem_limit_bytes=28 * 1024 * 1024
        ),
    )(*operands)


def fits(n, width, size, cut, hidden_all, experts, rows):
    return (
        n % 2 == 0
        and n <= 128
        and experts == n
        and width % (128 * n) == 0
        and hidden_all % (16 * n) == 0
        and size == 128
        and size % cut == 0
        and cut % 16 == 0
        and rows == 8
    )


def pick(n, *args):
    tokens, query_weight, memory_state = args[0], args[2], args[10]
    experts, hidden_all = args[18].shape[0] * n, args[21].shape[1]
    if fits(
        n, tokens.shape[1], memory_state.shape[3], query_weight.shape[1], hidden_all, experts,
        tokens.shape[0],
    ):
        return fused_shards(n, *args)
    return shards(*args)


def solution(mesh):
    placed = (
        P(("grp", "ep"), None),
        P(),
        P(None, "ep"),
        P(None, "ep"),
        P(None, "ep"),
        P(None, "ep"),
        P(),
        P(),
        P(),
        P(),
        P(("grp", "ep"), None, None, None),
        P(("grp", "ep"), None, None),
        P(("grp", "ep"), None),
        P(),
        P("ep", None),
        P(),
        P(("grp", "ep"), None),
        P(("grp", "ep"), None),
        P("ep", None, None),
        P("ep", None, None),
        P("ep", None, None),
        P("ep", None),
        P("ep", None),
        P(None, "ep"),
    )
    return jax.shard_map(
        functools.partial(pick, mesh.shape["ep"]),
        mesh=mesh,
        in_specs=placed,
        out_specs=(
            P(("grp", "ep"), None),
            P(("grp", "ep"), None, None, None),
            P(("grp", "ep"), None, None),
            P(("grp", "ep"), None),
        ),
        check_vma=False,
    )
```

```python
import jax
import jax.numpy as jnp
from jax import lax
from jax.experimental import pallas as pl
from jax.experimental.pallas import tpu as pltpu
from jax.sharding import PartitionSpec as P
import functools

epsilon = 1e-06


def rms_scale(values, gain):
    return (
        values
        * lax.rsqrt(jnp.mean(values * values, axis=-1, keepdims=True) + epsilon)
        * gain.astype(jnp.float32)
    )


def cell_step(
    normed,
    query,
    key_proj,
    value_proj,
    outgate,
    igate_weight,
    fgate_weight,
    igate_bias,
    fgate_bias,
    memory_state,
    norm_state,
    max_state,
    head_gain,
):
    row_count, head_count = max_state.shape
    head_size = memory_state.shape[-1]
    input_gate = jnp.dot(normed, igate_weight, preferred_element_type=jnp.float32) + igate_bias
    forget_log = jax.nn.log_sigmoid(
        jnp.dot(normed, fgate_weight, preferred_element_type=jnp.float32) + fgate_bias
    )
    query_heads = query.astype(jnp.float32).reshape(row_count, head_count, head_size)
    key_heads = key_proj.astype(jnp.float32).reshape(
        row_count, head_count, head_size
    ) * head_size ** (-0.5)
    value_heads = value_proj.astype(jnp.float32).reshape(row_count, head_count, head_size)
    max_next = jnp.maximum(forget_log + max_state, input_gate)
    decay_rate = jnp.exp(forget_log + max_state - max_next)
    injected = jnp.exp(input_gate - max_next)
    memory_next = decay_rate[:, :, None, None] * memory_state + injected[:, :, None, None] * (
        key_heads[:, :, :, None] * value_heads[:, :, None, :]
    )
    norm_next = decay_rate[:, :, None] * norm_state + injected[:, :, None] * key_heads
    numerator = jnp.einsum(
        "shd,shde->she", query_heads, memory_next, precision=lax.Precision.HIGHEST
    )
    denominator = jnp.maximum(
        jnp.abs(jnp.sum(query_heads * norm_next, axis=-1)), jnp.exp(-max_next)
    )
    readout = numerator / denominator[:, :, None]
    readout = rms_scale(readout, head_gain.reshape(head_count, head_size))
    gated = readout.reshape(row_count, head_count * head_size) * jax.nn.sigmoid(
        outgate.astype(jnp.float32)
    )
    return (gated.astype(jnp.bfloat16), memory_next, norm_next, max_next)


def shards(
    tokens,
    first_gain,
    query_weight,
    key_weight,
    value_weight,
    outgate_weight,
    igate_weight,
    fgate_weight,
    igate_bias,
    fgate_bias,
    memory_state,
    norm_state,
    max_state,
    head_gain,
    out_weight,
    second_gain,
    expert_ids,
    route_weight,
    expert_gate,
    expert_up,
    expert_down,
    shared_gate,
    shared_up,
    shared_down,
):
    own_rows = tokens.shape[0]
    devices = lax.axis_size("ep")
    top_count = expert_ids.shape[1]
    capacity = max(2, 2 * own_rows * top_count // devices)
    inputs = tokens.astype(jnp.float32)
    normed = rms_scale(inputs, first_gain).astype(jnp.bfloat16)
    block_rows = lax.all_gather(normed, "ep", axis=0, tiled=True)
    columns = jnp.stack(
        [
            jnp.dot(block_rows, matrix, preferred_element_type=jnp.float32).astype(jnp.bfloat16)
            for matrix in (query_weight, key_weight, value_weight, outgate_weight)
        ]
    )
    projected = lax.all_to_all(columns, "ep", split_axis=1, concat_axis=2, tiled=True)
    gated, memory_next, norm_next, max_next = cell_step(
        normed,
        projected[0],
        projected[1],
        projected[2],
        projected[3],
        igate_weight,
        fgate_weight,
        igate_bias,
        fgate_bias,
        memory_state,
        norm_state,
        max_state,
        head_gain,
    )
    picked = gated
    mix_sums = jnp.dot(
        picked,
        lax.all_gather(out_weight, "ep", axis=0, tiled=True),
        preferred_element_type=jnp.float32,
    )
    stream = inputs + mix_sums.astype(jnp.bfloat16).astype(jnp.float32)
    normed_two = rms_scale(stream, second_gain).astype(jnp.bfloat16)
    block_rows = (
        lax.all_gather(shared_gate, "ep", axis=0, tiled=True),
        lax.all_gather(shared_up, "ep", axis=0, tiled=True),
    )
    picked = normed_two
    gate_shared = jnp.dot(picked, block_rows[0], preferred_element_type=jnp.float32)
    up_shared = jnp.dot(picked, block_rows[1], preferred_element_type=jnp.float32)
    hidden_shared = (jax.nn.silu(gate_shared) * up_shared).astype(jnp.bfloat16)
    shared_result = jnp.dot(
        hidden_shared,
        lax.all_gather(shared_down, "ep", axis=1, tiled=True),
        preferred_element_type=jnp.float32,
    )
    choose = (expert_ids[:, :, None] == jnp.arange(devices, dtype=jnp.int32)[None, None, :]).astype(
        jnp.int32
    )
    counted = jnp.sum(choose, axis=1)
    ranking = jnp.cumsum(counted, axis=0) - counted
    slot_index = jnp.sum(choose * ranking[:, None, :], axis=2)
    slot_ids = jnp.arange(capacity, dtype=jnp.int32)
    selector = counted.T[:, None, :] * (ranking.T[:, None, :] == slot_ids[None, :, None]).astype(
        jnp.int32
    )
    outgoing = jnp.einsum(
        "ecr,rd->ecd", selector.astype(jnp.bfloat16), normed_two, preferred_element_type=jnp.float32
    ).astype(jnp.bfloat16)
    arrived = lax.all_to_all(outgoing, "ep", split_axis=0, concat_axis=0, tiled=True)
    sources, slots, width = arrived.shape
    flat_rows = arrived.reshape(sources * slots, width)
    gate_sums = jnp.dot(flat_rows, expert_gate[0], preferred_element_type=jnp.float32)
    up_sums = jnp.dot(flat_rows, expert_up[0], preferred_element_type=jnp.float32)
    hidden = (jax.nn.silu(gate_sums) * up_sums).astype(jnp.bfloat16)
    result = jnp.dot(hidden, expert_down[0], preferred_element_type=jnp.float32).astype(
        jnp.bfloat16
    )
    results = lax.all_to_all(
        result.reshape(sources, slots, width), "ep", split_axis=0, concat_axis=0, tiled=True
    )
    flat_results = results.reshape(devices * capacity, results.shape[2])
    picked_results = flat_results[expert_ids * capacity + slot_index]
    routed = jnp.sum(route_weight[:, :, None] * picked_results.astype(jnp.float32), axis=1)
    mixed_out = (stream + routed + shared_result).astype(jnp.bfloat16)
    return (mixed_out, memory_next, norm_next, max_next)


ANY, VMEM = pl.ANY, pltpu.VMEM
F32, BF16 = jnp.float32, jnp.bfloat16


def across(left, right):
    return lax.dot_general(left, right, (((1,), (1,)), ((), ())), preferred_element_type=F32)


def turned_dot(left, right):
    return lax.dot_general(
        left.astype(BF16),
        right.astype(BF16),
        (((0,), (0,)), ((), ())),
        preferred_element_type=F32,
    )


def in_line(gain):
    held = gain[...].astype(F32)
    return jnp.concatenate([held[i : i + 1] for i in range(held.shape[0])], axis=1)


def offsets(chips):
    ring = chips // 2
    steps = [(step, flip) for step in range(ring) for flip in (1, 0) if step or flip]
    return sorted(steps, key=lambda o: -(min(o[0], ring - o[0]) + o[1]))


def fused(n, *refs):
    (tokens, first_gain, query_weight, key_weight, value_weight, outgate_weight, igate_weight,
     fgate_weight, igate_bias, fgate_bias, memory_state, norm_state, max_state, head_gain,
     out_weight, second_gain, expert_ids, route_weight, expert_gate, expert_up, expert_down,
     shared_gate, shared_up, shared_down,
     mixed_out, memory_next, norm_next, max_next,
     gain_one, gain_two, bias, gates_in, norm_in, max_in, gain_head, ids, route, sgate, sup, sdown,
     out_own, proj, wide, down, tok_all, table, normed, column_send, column_recv, gated_all,
     ow_all, mix_all, streamed, shared_send, shared_recv, sdown_recv, part, part_send, sum_recv,
     local_sem, memory_sem, send_sem, recv_sem, pair_send, pair_recv) = refs
    rows, width = tokens.shape
    heads, size = memory_state.shape[1], memory_state.shape[3]
    cut = query_weight.shape[0]
    chips = n // 2
    hidden = sgate.shape[1] // chips
    block = width // chips
    group = chips * rows
    top_count = expert_ids.shape[1]
    ring = chips // 2
    me = lax.axis_index("ep")
    side, chip = me % 2, me // 2
    partner = me + 1 - 2 * side
    order = offsets(chips)

    def to_chip(k):
        step, flip = order[k]
        return 2 * ((chip // 2 + step) % ring) + (chip + flip) % 2

    def from_chip(k):
        step, flip = order[k]
        return 2 * ((chip // 2 + ring - step) % ring) + (chip + flip) % 2

    barrier = pltpu.get_barrier_semaphore()
    for k in range(len(order)):
        pl.semaphore_signal(
            barrier,
            inc=1,
            device_id={"ep": 2 * to_chip(k) + side},
            device_id_type=pl.DeviceIdType.MESH,
        )
    pl.semaphore_signal(
        barrier, inc=1, device_id={"ep": partner}, device_id_type=pl.DeviceIdType.MESH
    )

    loads = []

    def load(source, target):
        copy = pltpu.make_async_copy(source, target, local_sem.at[len(loads)])
        copy.start()
        loads.append(copy)
        return copy

    token_load = load(tokens, tok_all.at[chip])
    gain_load = load(first_gain, gain_one)
    early = [
        load(igate_weight, gates_in.at[0]),
        load(fgate_weight, gates_in.at[1]),
        load(igate_bias, bias.at[0]),
        load(fgate_bias, bias.at[1]),
        load(max_state, max_in),
        load(expert_ids, ids),
        load(route_weight, route),
        load(shared_gate, sgate),
        load(shared_up, sup),
        load(shared_down, sdown),
        load(norm_state, norm_in),
        load(head_gain, gain_head),
        load(second_gain, gain_two),
    ]
    weights = (query_weight, key_weight, value_weight, outgate_weight)
    proj_loads = [load(matrix, proj.at[i, side]) for i, matrix in enumerate(weights)]
    out_load = load(out_weight, out_own)
    memory_loads = []
    for h in range(heads):
        copy = pltpu.make_async_copy(
            memory_state.at[:, h], memory_next.at[:, h], memory_sem.at[h]
        )
        copy.start()
        memory_loads.append(copy)
    columns_own = pl.ds(pl.multiple_of(chip * block, block), block)
    late = [
        load(out_weight.at[:, columns_own], ow_all.at[me]),
        load(expert_gate.at[0], wide.at[side, 0]),
        load(expert_up.at[0], wide.at[side, 1]),
        load(expert_down.at[0], down.at[side]),
    ]
    token_load.wait()
    unsent = []

    def spread(which, source, target):
        copies = []
        for k in range(len(order)):
            there = to_chip(k)
            copy = pltpu.make_async_remote_copy(
                src_ref=source(there),
                dst_ref=target,
                send_sem=send_sem.at[which, k],
                recv_sem=recv_sem.at[which, k],
                device_id={"ep": 2 * there + side},
                device_id_type=pl.DeviceIdType.MESH,
            )
            copy.start()
            copies.append(copy)
        unsent.extend(copies)
        return copies

    pairs = []

    def push(source, target):
        copy = pltpu.make_async_remote_copy(
            src_ref=source,
            dst_ref=target,
            send_sem=pair_send.at[len(pairs)],
            recv_sem=pair_recv.at[len(pairs)],
            device_id={"ep": partner},
            device_id_type=pl.DeviceIdType.MESH,
        )
        copy.start()
        pairs.append(copy)
        return copy

    pl.semaphore_wait(barrier, len(order) + 1)
    first = spread(0, lambda there: tok_all.at[chip], tok_all.at[chip])
    proj_pushes = [push(matrix, proj.at[i, side]) for i, matrix in enumerate(weights)]

    gain_load.wait()
    gain = in_line(gain_one)

    def norm_rows(source):
        values = rms_scale(tok_all[source].astype(F32), gain)
        normed[pl.ds(pl.multiple_of(source * rows, rows), rows), :] = values
        return values.astype(BF16)

    own = norm_rows(chip)
    for copy in early:
        copy.wait()
    lanes = lax.broadcasted_iota(jnp.int32, (rows, 128), 1)
    routes = jnp.zeros((rows, 128), F32)
    for t in range(top_count):
        routes = routes + jnp.where(ids[:, t : t + 1] == lanes, route[:, t : t + 1], 0.0)
    table[chip] = routes
    for i, matrix in enumerate((sgate, sup)):
        turned = matrix[...].astype(F32).T.reshape(chips, hidden, matrix.shape[0])
        shared_send[:, i * hidden : (i + 1) * hidden, :] = turned.astype(BF16)
    input_gate = across(own, gates_in[0]) + bias[0]
    forget_log = jax.nn.log_sigmoid(across(own, gates_in[1]) + bias[1])
    kept = forget_log + max_in[...]
    top = jnp.maximum(kept, input_gate)
    max_next[...] = top
    decay_rate = jnp.exp(kept - top)
    injected = jnp.exp(input_gate - top)
    floor = jnp.exp(-top)
    for copy in proj_loads:
        copy.wait()
    for copy in proj_pushes:
        copy.wait_recv()

    for k in reversed(range(len(order))):
        first[k].wait_recv()
        norm_rows(from_chip(k))

    columns = across(normed[...].astype(BF16), proj[...].reshape(8 * cut, width))
    column_send[...] = columns.reshape(chips, rows, 8 * cut).astype(BF16)
    second = spread(1, lambda there: column_send.at[there], column_recv.at[chip])
    column_recv[chip] = column_send[chip]
    out_load.wait()

    def out_columns(there):
        return out_own.at[:, pl.ds(pl.multiple_of(there * block, block), block)]

    out_spread = spread(2, out_columns, ow_all.at[me])
    table_spread = spread(3, lambda there: table.at[chip], table.at[chip])
    out_pushes = [push(out_columns(chip), ow_all.at[me])]
    expert_pushes = [
        push(expert_gate.at[0], wide.at[side, 0]),
        push(expert_up.at[0], wide.at[side, 1]),
        push(expert_down.at[0], down.at[side]),
    ]
    for k in range(len(order)):
        second[k].wait_recv()

    place = lax.broadcasted_iota(jnp.int32, (rows, rows * size), 1) // size
    diagonal = place == lax.broadcasted_iota(jnp.int32, (rows, rows * size), 0)
    ones = jnp.where(diagonal, 1.0, 0.0)
    blocks = jnp.concatenate([ones, jnp.zeros_like(ones)], axis=0)
    for h in range(heads):
        piece = column_recv[h].astype(F32)
        query, keyed, valued, outgate = [piece[:, i * size : (i + 1) * size] for i in range(4)]
        scale = injected[:, h : h + 1] * size ** (-0.5)
        decay = jnp.broadcast_to(decay_rate[:, h : h + 1], (rows, size))
        norm = decay * norm_in[:, h, :] + scale * keyed
        norm_next[:, h, :] = norm
        bottom = jnp.maximum(
            jnp.abs(jnp.sum(query * norm, axis=-1, keepdims=True)), floor[:, h : h + 1]
        )
        spread_value = jnp.where(diagonal, jnp.concatenate([scale * valued] * rows, axis=1), 0.0)
        high = spread_value.astype(BF16).astype(F32)
        outer = turned_dot(
            jnp.concatenate([keyed, keyed], axis=0),
            jnp.concatenate([high, spread_value - high], axis=0),
        )
        wide_query = turned_dot(jnp.concatenate([query, query * 0.0], axis=0), blocks)
        memory_loads[h].wait()
        tops = []
        for s in range(rows):
            cell = (
                decay[s : s + 1, :] * memory_next[s, h] + outer[:, s * size : (s + 1) * size]
            )
            memory_next[s, h] = cell
            tops.append(
                jnp.sum(wide_query[:, s * size : (s + 1) * size] * cell, axis=0, keepdims=True)
            )
        readout = jnp.concatenate(tops, axis=0) / bottom
        readout = rms_scale(readout, gain_head[h : h + 1, :])
        gated_all[chip, :, h * size : (h + 1) * size] = (
            readout * jax.nn.sigmoid(outgate)
        ).astype(BF16)

    third = spread(4, lambda there: gated_all.at[chip], gated_all.at[chip])
    for copy in late:
        copy.wait()
    for k in range(len(order)):
        out_spread[k].wait_recv()
        source = 2 * from_chip(k) + side
        out_pushes.append(push(ow_all.at[source], ow_all.at[source]))
    shared_spread = spread(5, lambda there: shared_send.at[there], shared_recv.at[me])
    shared_recv[me] = shared_send[chip]
    down_spread = spread(6, lambda there: sdown.at[there], sdown_recv.at[me])
    sdown_recv[me] = sdown[chip]
    shared_pushes = [
        push(shared_send.at[chip], shared_recv.at[me]),
        push(sdown.at[chip], sdown_recv.at[me]),
    ]
    for copy in out_pushes:
        copy.wait_recv()
    for k in range(len(order)):
        third[k].wait_recv()

    def flat(buffer):
        held = buffer[...].astype(F32)
        return held.reshape(group, held.shape[2])

    mix = jnp.dot(
        flat(gated_all).astype(BF16),
        ow_all[...].reshape(n * cut, block),
        preferred_element_type=F32,
    )
    mix_all[chip] = mix.astype(BF16)
    fourth = spread(7, lambda there: mix_all.at[chip], mix_all.at[chip])
    for k in range(len(order)):
        shared_spread[k].wait_recv()
        down_spread[k].wait_recv()
        source = 2 * from_chip(k) + side
        shared_pushes.append(push(shared_recv.at[source], shared_recv.at[source]))
        shared_pushes.append(push(sdown_recv.at[source], sdown_recv.at[source]))
    for k in range(len(order)):
        table_spread[k].wait_recv()
    weights_all = flat(table)
    expert_lane = lax.broadcasted_iota(jnp.int32, weights_all.shape, 1)
    for copy in shared_pushes + expert_pushes:
        copy.wait_recv()
    shared_wide = jnp.concatenate([shared_recv[i] for i in range(n)], axis=1)
    shared_rows = jnp.concatenate([sdown_recv[i] for i in range(n)], axis=1)
    for k in range(len(order)):
        fourth[k].wait_recv()

    stream = flat(tok_all) + jnp.concatenate(
        [mix_all[c].astype(F32) for c in range(chips)], axis=1
    )
    streamed[...] = stream.reshape(chips, rows, width)
    rows_two = rms_scale(stream, in_line(gain_two)).astype(BF16)
    both = across(rows_two, shared_wide)
    shared_hidden = (jax.nn.silu(both[:, :hidden]) * both[:, hidden:]).astype(BF16)
    value = jnp.dot(shared_hidden, shared_rows, preferred_element_type=F32)
    for e in range(2):
        gate_sums = jnp.dot(rows_two, wide[e, 0], preferred_element_type=F32)
        up_sums = jnp.dot(rows_two, wide[e, 1], preferred_element_type=F32)
        weight = jnp.sum(
            jnp.where(expert_lane == 2 * chip + e, weights_all, 0.0), axis=1, keepdims=True
        )
        own_hidden = (jax.nn.silu(gate_sums) * up_sums * weight).astype(BF16)
        value = value + jnp.dot(own_hidden, down[e], preferred_element_type=F32)
    part[...] = value.reshape(chips, rows, width)
    part_send[...] = value.reshape(chips, rows, width).astype(BF16)
    fifth = spread(8, lambda there: part_send.at[there], sum_recv.at[chip])
    total = streamed[chip] + part[chip]
    for k in reversed(range(len(order))):
        fifth[k].wait_recv()
        total = total + sum_recv[from_chip(k)].astype(F32)
    mixed_out[...] = total.astype(BF16)

    for copy in unsent + pairs:
        copy.wait_send()


def flush(*refs):
    sources, targets, sems = refs[:4], refs[4:8], refs[8]
    copies = []
    for i in (1, 2, 0, 3):
        if i == 1:
            for s in range(sources[i].shape[0]):
                copies.append((sources[i].at[s], targets[i].at[s]))
        else:
            copies.append((sources[i], targets[i]))
    started = []
    for i, (source, target) in enumerate(copies):
        copy = pltpu.make_async_copy(source, target, sems.at[i])
        copy.start()
        started.append(copy)
    for copy in started:
        copy.wait()


def fused_shards(n, *args):
    (tokens, first_gain, query_weight, key_weight, value_weight, outgate_weight, igate_weight,
     fgate_weight, igate_bias, fgate_bias, memory_state, norm_state, max_state, head_gain,
     out_weight, second_gain, expert_ids, route_weight, expert_gate, expert_up, expert_down,
     shared_gate, shared_up, shared_down) = args
    rows, width = tokens.shape
    heads, size = memory_state.shape[1], memory_state.shape[3]
    cut = query_weight.shape[1]
    chips = n // 2
    hidden = shared_gate.shape[1] // chips
    inner = expert_gate.shape[2]
    top_count = expert_ids.shape[1]
    deep = shared_gate.shape[0]
    lean = shared_down.shape[1]
    operands = (
        tokens, first_gain.reshape(-1, 128), query_weight.T, key_weight.T, value_weight.T,
        outgate_weight.T, igate_weight.T, fgate_weight.T, igate_bias.reshape(1, -1), fgate_bias.reshape(1, -1),
        memory_state, norm_state, max_state, head_gain.reshape(heads, size), out_weight,
        second_gain.reshape(-1, 128), expert_ids, route_weight, expert_gate, expert_up, expert_down,
        shared_gate, shared_up, shared_down.reshape(chips, hidden, lean),
    )
    operands = [pltpu.with_memory_space_constraint(x, pltpu.HBM) for x in operands]
    dma = pltpu.SemaphoreType.DMA
    results = (
        jax.ShapeDtypeStruct((rows, width), BF16),
        jax.ShapeDtypeStruct(memory_state.shape, F32),
        jax.ShapeDtypeStruct(norm_state.shape, F32),
        jax.ShapeDtypeStruct(max_state.shape, F32),
    )
    inside = pl.pallas_call(
        functools.partial(fused, n),
        out_shape=results,
        in_specs=[pl.BlockSpec(memory_space=pltpu.HBM)] * len(operands),
        out_specs=tuple(pl.BlockSpec(memory_space=VMEM) for _ in results),
        scratch_shapes=[
            VMEM((width // 128, 128), BF16),
            VMEM((width // 128, 128), BF16),
            VMEM((2, 1, heads), F32),
            VMEM((2, heads, width), BF16),
            VMEM(norm_state.shape, F32),
            VMEM(max_state.shape, F32),
            VMEM((heads, size), BF16),
            VMEM((rows, top_count), jnp.int32),
            VMEM((rows, top_count), F32),
            VMEM(shared_gate.shape, BF16),
            VMEM(shared_up.shape, BF16),
            VMEM((chips, hidden, lean), BF16),
            VMEM(out_weight.shape, BF16),
            VMEM((4, 2, cut, width), BF16),
            VMEM((2, 2, width, inner), BF16),
            VMEM((2, inner, width), BF16),
            VMEM((chips, rows, width), BF16),
            VMEM((chips, rows, 128), F32),
            VMEM((chips * rows, width), F32),
            VMEM((chips, rows, 8 * cut), BF16),
            VMEM((chips, rows, 8 * cut), BF16),
            VMEM((chips, rows, heads * size), BF16),
            VMEM((n, cut, width // chips), BF16),
            VMEM((chips, chips * rows, width // chips), BF16),
            VMEM((chips, rows, width), F32),
            VMEM((chips, 2 * hidden, deep), BF16),
            VMEM((n, 2 * hidden, deep), BF16),
            VMEM((n, hidden, lean), BF16),
            VMEM((chips, rows, width), F32),
            VMEM((chips, rows, width), BF16),
            VMEM((chips, rows, width), BF16),
            dma((32,)),
            dma((heads,)),
            dma((9, chips)),
            dma((9, chips)),
            dma((10 + 3 * chips,)),
            dma((10 + 3 * chips,)),
        ],
        compiler_params=pltpu.CompilerParams(
            collective_id=0, has_side_effects=True, vmem_limit_bytes=36 * 1024 * 1024
        ),
    )(*operands)
    return pl.pallas_call(
        flush,
        out_shape=results,
        in_specs=[pl.BlockSpec(memory_space=VMEM)] * 4,
        out_specs=tuple(pl.BlockSpec(memory_space=pltpu.HBM) for _ in results),
        scratch_shapes=[dma((rows + 3,))],
        compiler_params=pltpu.CompilerParams(vmem_limit_bytes=1024 * 1024),
    )(*[pltpu.with_memory_space_constraint(x, VMEM) for x in inside])


def fits(n, width, size, heads, cut, hidden_all, experts, rows):
    chips = n // 2
    return (
        n % 4 == 0
        and experts == n
        and heads == chips
        and 2 * cut == size
        and size == 128
        and width % (128 * n) == 0
        and hidden_all % (16 * chips) == 0
        and rows == 8
    )


def pick(n, *args):
    tokens, query_weight, memory_state = args[0], args[2], args[10]
    experts, hidden_all = args[18].shape[0] * n, args[21].shape[1]
    if fits(
        n, tokens.shape[1], memory_state.shape[3], memory_state.shape[1], query_weight.shape[1],
        hidden_all, experts, tokens.shape[0],
    ):
        return fused_shards(n, *args)
    return shards(*args)


def solution(mesh):
    placed = (
        P(("grp", "ep"), None),
        P(),
        P(None, "ep"),
        P(None, "ep"),
        P(None, "ep"),
        P(None, "ep"),
        P(),
        P(),
        P(),
        P(),
        P(("grp", "ep"), None, None, None),
        P(("grp", "ep"), None, None),
        P(("grp", "ep"), None),
        P(),
        P("ep", None),
        P(),
        P(("grp", "ep"), None),
        P(("grp", "ep"), None),
        P("ep", None, None),
        P("ep", None, None),
        P("ep", None, None),
        P("ep", None),
        P("ep", None),
        P(None, "ep"),
    )
    return jax.shard_map(
        functools.partial(pick, mesh.shape["ep"]),
        mesh=mesh,
        in_specs=placed,
        out_specs=(
            P(("grp", "ep"), None),
            P(("grp", "ep"), None, None, None),
            P(("grp", "ep"), None, None),
            P(("grp", "ep"), None),
        ),
        check_vma=False,
    )
```

```python
import jax
import jax.numpy as jnp
from jax import lax
from jax.experimental import pallas as pl
from jax.experimental.pallas import tpu as pltpu
from jax.sharding import PartitionSpec as P
import functools

epsilon = 1e-06


def rms_scale(values, gain):
    return (
        values
        * lax.rsqrt(jnp.mean(values * values, axis=-1, keepdims=True) + epsilon)
        * gain.astype(jnp.float32)
    )


def cell_step(
    normed,
    query,
    key_proj,
    value_proj,
    outgate,
    igate_weight,
    fgate_weight,
    igate_bias,
    fgate_bias,
    memory_state,
    norm_state,
    max_state,
    head_gain,
):
    row_count, head_count = max_state.shape
    head_size = memory_state.shape[-1]
    input_gate = jnp.dot(normed, igate_weight, preferred_element_type=jnp.float32) + igate_bias
    forget_log = jax.nn.log_sigmoid(
        jnp.dot(normed, fgate_weight, preferred_element_type=jnp.float32) + fgate_bias
    )
    query_heads = query.astype(jnp.float32).reshape(row_count, head_count, head_size)
    key_heads = key_proj.astype(jnp.float32).reshape(
        row_count, head_count, head_size
    ) * head_size ** (-0.5)
    value_heads = value_proj.astype(jnp.float32).reshape(row_count, head_count, head_size)
    max_next = jnp.maximum(forget_log + max_state, input_gate)
    decay_rate = jnp.exp(forget_log + max_state - max_next)
    injected = jnp.exp(input_gate - max_next)
    memory_next = decay_rate[:, :, None, None] * memory_state + injected[:, :, None, None] * (
        key_heads[:, :, :, None] * value_heads[:, :, None, :]
    )
    norm_next = decay_rate[:, :, None] * norm_state + injected[:, :, None] * key_heads
    numerator = jnp.einsum(
        "shd,shde->she", query_heads, memory_next, precision=lax.Precision.HIGHEST
    )
    denominator = jnp.maximum(
        jnp.abs(jnp.sum(query_heads * norm_next, axis=-1)), jnp.exp(-max_next)
    )
    readout = numerator / denominator[:, :, None]
    readout = rms_scale(readout, head_gain.reshape(head_count, head_size))
    gated = readout.reshape(row_count, head_count * head_size) * jax.nn.sigmoid(
        outgate.astype(jnp.float32)
    )
    return (gated.astype(jnp.bfloat16), memory_next, norm_next, max_next)


def shards(
    tokens,
    first_gain,
    query_weight,
    key_weight,
    value_weight,
    outgate_weight,
    igate_weight,
    fgate_weight,
    igate_bias,
    fgate_bias,
    memory_state,
    norm_state,
    max_state,
    head_gain,
    out_weight,
    second_gain,
    expert_ids,
    route_weight,
    expert_gate,
    expert_up,
    expert_down,
    shared_gate,
    shared_up,
    shared_down,
):
    own_rows = tokens.shape[0]
    devices = lax.axis_size("ep")
    top_count = expert_ids.shape[1]
    capacity = max(2, 2 * own_rows * top_count // devices)
    inputs = tokens.astype(jnp.float32)
    normed = rms_scale(inputs, first_gain).astype(jnp.bfloat16)
    block_rows = lax.all_gather(normed, "ep", axis=0, tiled=True)
    columns = jnp.stack(
        [
            jnp.dot(block_rows, matrix, preferred_element_type=jnp.float32).astype(jnp.bfloat16)
            for matrix in (query_weight, key_weight, value_weight, outgate_weight)
        ]
    )
    projected = lax.all_to_all(columns, "ep", split_axis=1, concat_axis=2, tiled=True)
    gated, memory_next, norm_next, max_next = cell_step(
        normed,
        projected[0],
        projected[1],
        projected[2],
        projected[3],
        igate_weight,
        fgate_weight,
        igate_bias,
        fgate_bias,
        memory_state,
        norm_state,
        max_state,
        head_gain,
    )
    picked = gated
    mix_sums = jnp.dot(
        picked,
        lax.all_gather(out_weight, "ep", axis=0, tiled=True),
        preferred_element_type=jnp.float32,
    )
    stream = inputs + mix_sums.astype(jnp.bfloat16).astype(jnp.float32)
    normed_two = rms_scale(stream, second_gain).astype(jnp.bfloat16)
    block_rows = (
        lax.all_gather(shared_gate, "ep", axis=0, tiled=True),
        lax.all_gather(shared_up, "ep", axis=0, tiled=True),
    )
    picked = normed_two
    gate_shared = jnp.dot(picked, block_rows[0], preferred_element_type=jnp.float32)
    up_shared = jnp.dot(picked, block_rows[1], preferred_element_type=jnp.float32)
    hidden_shared = (jax.nn.silu(gate_shared) * up_shared).astype(jnp.bfloat16)
    shared_result = jnp.dot(
        hidden_shared,
        lax.all_gather(shared_down, "ep", axis=1, tiled=True),
        preferred_element_type=jnp.float32,
    )
    choose = (expert_ids[:, :, None] == jnp.arange(devices, dtype=jnp.int32)[None, None, :]).astype(
        jnp.int32
    )
    counted = jnp.sum(choose, axis=1)
    ranking = jnp.cumsum(counted, axis=0) - counted
    slot_index = jnp.sum(choose * ranking[:, None, :], axis=2)
    slot_ids = jnp.arange(capacity, dtype=jnp.int32)
    selector = counted.T[:, None, :] * (ranking.T[:, None, :] == slot_ids[None, :, None]).astype(
        jnp.int32
    )
    outgoing = jnp.einsum(
        "ecr,rd->ecd", selector.astype(jnp.bfloat16), normed_two, preferred_element_type=jnp.float32
    ).astype(jnp.bfloat16)
    arrived = lax.all_to_all(outgoing, "ep", split_axis=0, concat_axis=0, tiled=True)
    sources, slots, width = arrived.shape
    flat_rows = arrived.reshape(sources * slots, width)
    gate_sums = jnp.dot(flat_rows, expert_gate[0], preferred_element_type=jnp.float32)
    up_sums = jnp.dot(flat_rows, expert_up[0], preferred_element_type=jnp.float32)
    hidden = (jax.nn.silu(gate_sums) * up_sums).astype(jnp.bfloat16)
    result = jnp.dot(hidden, expert_down[0], preferred_element_type=jnp.float32).astype(
        jnp.bfloat16
    )
    results = lax.all_to_all(
        result.reshape(sources, slots, width), "ep", split_axis=0, concat_axis=0, tiled=True
    )
    flat_results = results.reshape(devices * capacity, results.shape[2])
    picked_results = flat_results[expert_ids * capacity + slot_index]
    routed = jnp.sum(route_weight[:, :, None] * picked_results.astype(jnp.float32), axis=1)
    mixed_out = (stream + routed + shared_result).astype(jnp.bfloat16)
    return (mixed_out, memory_next, norm_next, max_next)


ANY, VMEM = pl.ANY, pltpu.VMEM
F32, BF16 = jnp.float32, jnp.bfloat16


def across(left, right):
    return lax.dot_general(left, right, (((1,), (1,)), ((), ())), preferred_element_type=F32)


def turned_dot(left, right):
    return lax.dot_general(
        left.astype(BF16),
        right.astype(BF16),
        (((0,), (0,)), ((), ())),
        preferred_element_type=F32,
    )


def in_line(gain):
    held = gain[...].astype(F32)
    return jnp.concatenate([held[i : i + 1] for i in range(held.shape[0])], axis=1)


def offsets(chips):
    ring = chips // 2
    steps = [(step, flip) for step in range(ring) for flip in (1, 0) if step or flip]
    return sorted(steps, key=lambda o: -(min(o[0], ring - o[0]) + o[1]))


def fused(n, *refs):
    (tokens, first_gain, query_weight, key_weight, value_weight, outgate_weight, igate_weight,
     fgate_weight, igate_bias, fgate_bias, memory_state, norm_state, max_state, head_gain,
     out_weight, second_gain, expert_ids, route_weight, expert_gate, expert_up, expert_down,
     shared_gate, shared_up, shared_down,
     mixed_out, memory_next, norm_next, max_next,
     gain_one, gain_two, bias, gates_in, norm_in, max_in, gain_head, ids, route, sgate, sup,
     out_own, proj, wide, down, tok_all, table, normed, column_send, column_recv, gated_all,
     ow_all, mix_all, streamed, pack_send, pack_recv, part, part_send, sum_recv, gain_rows, sums_all,
     local_sem, memory_sem, send_sem, recv_sem, pair_send, pair_recv, twin_send, twin_recv) = refs
    rows, width = tokens.shape
    heads, size = memory_state.shape[1], memory_state.shape[3]
    cut = query_weight.shape[0]
    chips = n // 2
    hidden = sgate.shape[1] // chips
    block = width // chips
    group = chips * rows
    top_count = expert_ids.shape[1]
    ring = chips // 2
    me = lax.axis_index("ep")
    plane = lax.axis_index("grp")
    other = 1 - plane
    side, chip = me % 2, me // 2
    partner = me + 1 - 2 * side
    order = offsets(chips)

    def to_chip(k):
        step, flip = order[k]
        return 2 * ((chip // 2 + step) % ring) + (chip + flip) % 2

    def from_chip(k):
        step, flip = order[k]
        return 2 * ((chip // 2 + ring - step) % ring) + (chip + flip) % 2

    barrier = pltpu.get_barrier_semaphore()
    for k in range(len(order)):
        pl.semaphore_signal(
            barrier,
            inc=1,
            device_id={"ep": 2 * to_chip(k) + side},
            device_id_type=pl.DeviceIdType.MESH,
        )
    pl.semaphore_signal(
        barrier, inc=1, device_id={"ep": partner}, device_id_type=pl.DeviceIdType.MESH
    )

    pl.semaphore_signal(
        barrier, inc=1, device_id={"grp": other}, device_id_type=pl.DeviceIdType.MESH
    )
    loads = []

    def load(source, target):
        copy = pltpu.make_async_copy(source, target, local_sem.at[len(loads)])
        copy.start()
        loads.append(copy)
        return copy

    token_load = load(tokens, tok_all.at[chip])
    gain_load = load(first_gain, gain_one)
    early = [
        load(igate_weight, gates_in.at[0]),
        load(fgate_weight, gates_in.at[1]),
        load(igate_bias, bias.at[0]),
        load(fgate_bias, bias.at[1]),
        load(max_state, max_in),
        load(expert_ids, ids),
        load(route_weight, route),
        load(shared_gate, sgate),
        load(shared_up, sup),
        load(shared_down.at[:, 0], pack_send.at[:, 0, hidden:]),
        load(shared_down.at[:, 1], pack_send.at[:, 1, hidden:]),
        load(norm_state, norm_in),
        load(head_gain, gain_head),
        load(second_gain, gain_two),
    ]
    weights = (query_weight, key_weight, value_weight, outgate_weight)
    proj_loads = [load(matrix, proj.at[i, side]) for i, matrix in enumerate(weights)]
    out_loads = [
        load(
            out_weight.at[i * cut // 2 : (i + 1) * cut // 2, pl.ds(c * block, block)],
            out_own.at[c, i],
        )
        for c in range(chips)
        for i in range(2)
    ]
    memory_loads = []
    for h in range(heads):
        copy = pltpu.make_async_copy(
            memory_state.at[:, h], memory_next.at[:, h], memory_sem.at[h]
        )
        copy.start()
        memory_loads.append(copy)
    late = [
        load(expert_gate.at[0], wide.at[side, 0]),
        load(expert_up.at[0], wide.at[side, 1]),
        load(expert_down.at[0], down.at[side]),
    ]
    token_load.wait()
    unsent = []

    def spread(which, source, target):
        copies = []
        for k in range(len(order)):
            there = to_chip(k)
            copy = pltpu.make_async_remote_copy(
                src_ref=source(there),
                dst_ref=target,
                send_sem=send_sem.at[which, k],
                recv_sem=recv_sem.at[which, k],
                device_id={"ep": 2 * there + side},
                device_id_type=pl.DeviceIdType.MESH,
            )
            copy.start()
            copies.append(copy)
        unsent.extend(copies)
        return copies

    twins = []

    def cross(source, target):
        copy = pltpu.make_async_remote_copy(
            src_ref=source,
            dst_ref=target,
            send_sem=twin_send.at[len(twins)],
            recv_sem=twin_recv.at[len(twins)],
            device_id={"grp": other},
            device_id_type=pl.DeviceIdType.MESH,
        )
        copy.start()
        twins.append(copy)
        return copy

    pairs = []

    def push(source, target):
        copy = pltpu.make_async_remote_copy(
            src_ref=source,
            dst_ref=target,
            send_sem=pair_send.at[len(pairs)],
            recv_sem=pair_recv.at[len(pairs)],
            device_id={"ep": partner},
            device_id_type=pl.DeviceIdType.MESH,
        )
        copy.start()
        pairs.append(copy)
        return copy

    drained = [0, 0, 0]

    def drain(keep=0):
        for i, held in enumerate((unsent, pairs, twins)):
            stop = len(held) - (keep if i == 0 else 0)
            for copy in held[drained[i] : stop]:
                copy.wait_send()
            drained[i] = stop

    pl.semaphore_wait(barrier, len(order) + 2)
    first = spread(0, lambda there: tok_all.at[chip], tok_all.at[chip])
    proj_pushes = [push(matrix, proj.at[i, side]) for i, matrix in enumerate(weights)]

    expert_pushes = [
        push(expert_gate.at[0], wide.at[side, 0]),
        push(expert_up.at[0], wide.at[side, 1]),
        push(expert_down.at[0], down.at[side]),
    ]
    gain_load.wait()
    gain = in_line(gain_one)

    def norm_rows(source):
        values = rms_scale(tok_all[source].astype(F32), gain)
        normed[pl.ds(pl.multiple_of(source * rows, rows), rows), :] = values
        return values.astype(BF16)

    own = norm_rows(chip)
    for copy in early:
        copy.wait()
    lanes = lax.broadcasted_iota(jnp.int32, (rows, rows * n), 1)
    mine = lanes // n == lax.broadcasted_iota(jnp.int32, (rows, rows * n), 0)
    routes = jnp.zeros((rows, rows * n), F32)
    for t in range(top_count):
        routes = routes + jnp.where(
            mine & (lanes % n == ids[:, t : t + 1]), route[:, t : t + 1], 0.0
        )
    table[chip] = jnp.sum(routes, axis=0, keepdims=True)
    for i, matrix in enumerate((sgate, sup)):
        turned = matrix[...].astype(F32).T.reshape(chips, hidden, matrix.shape[0])
        pack_send[:, i, :hidden, :] = turned.astype(BF16)
    input_gate = across(own, gates_in[0]) + bias[0]
    forget_log = jax.nn.log_sigmoid(across(own, gates_in[1]) + bias[1])
    kept = forget_log + max_in[...]
    top = jnp.maximum(kept, input_gate)
    max_next[...] = top
    decay_rate = jnp.exp(kept - top)
    injected = jnp.exp(input_gate - top)
    floor = jnp.exp(-top)
    for copy in proj_loads:
        copy.wait()
    for copy in proj_pushes:
        copy.wait_recv()

    for k in reversed(range(len(order))):
        first[k].wait_recv()
        norm_rows(from_chip(k))

    columns = across(normed[...].astype(BF16), proj[...].reshape(8 * cut, width))
    column_send[...] = columns.reshape(chips, rows, 8 * cut).astype(BF16)
    second = spread(1, lambda there: column_send.at[there], column_recv.at[chip])
    column_recv[chip] = column_send[chip]
    for copy in out_loads:
        copy.wait()
    out_spread = spread(2, lambda there: out_own.at[there, plane], ow_all.at[me, plane])
    table_spread = spread(3, lambda there: table.at[chip], table.at[chip])
    near_pushes = [push(out_own.at[chip], ow_all.at[me]), push(pack_send.at[chip], pack_recv.at[me])]
    ow_all[me] = out_own[chip]
    pack_recv[me] = pack_send[chip]
    out_pushes, pack_pushes, out_twins, pack_twins = [], [], [], []

    def forward(copies, buffer, crossed, pushed):
        for k in range(len(order)):
            copies[k].wait_recv()
            held = buffer.at[2 * from_chip(k) + side, plane]
            crossed.append(cross(held, held))
            pushed.append(push(held, held))

    def settle(crossed, buffer, pushed):
        for k in range(len(order)):
            crossed[k].wait_recv()
            held = buffer.at[2 * from_chip(k) + side, other]
            pushed.append(push(held, held))

    for copy in memory_loads:
        copy.wait()
    for k in range(len(order)):
        second[k].wait_recv()

    place = lax.broadcasted_iota(jnp.int32, (rows, rows * size), 1) // size
    diagonal = place == lax.broadcasted_iota(jnp.int32, (rows, rows * size), 0)
    for h in range(heads):
        piece = column_recv[h].astype(F32)
        query, keyed, valued, outgate = [piece[:, i * size : (i + 1) * size] for i in range(4)]
        scale = injected[:, h : h + 1] * size ** (-0.5)
        decay = jnp.broadcast_to(decay_rate[:, h : h + 1], (rows, size))
        norm = decay * norm_in[:, h, :] + scale * keyed
        norm_next[:, h, :] = norm
        bottom = jnp.maximum(
            jnp.abs(jnp.sum(query * norm, axis=-1, keepdims=True)), floor[:, h : h + 1]
        )
        spread_value = jnp.where(diagonal, jnp.concatenate([scale * valued] * rows, axis=1), 0.0)
        high = spread_value.astype(BF16).astype(F32)
        outer = turned_dot(
            jnp.concatenate([keyed, keyed], axis=0),
            jnp.concatenate([high, spread_value - high], axis=0),
        )
        query_columns = query.T
        tops = []
        for s in range(rows):
            cell = (
                decay[s : s + 1, :] * memory_next[s, h] + outer[:, s * size : (s + 1) * size]
            )
            memory_next[s, h] = cell
            tops.append(jnp.sum(query_columns[:, s : s + 1] * cell, axis=0, keepdims=True))
        readout = jnp.concatenate(tops, axis=0) / bottom
        readout = rms_scale(readout, gain_head[h : h + 1, :])
        gated_all[chip, :, h * size : (h + 1) * size] = (
            readout * jax.nn.sigmoid(outgate)
        ).astype(BF16)
        if h == heads // 2:
            forward(out_spread, ow_all, out_twins, out_pushes)

    third = spread(4, lambda there: gated_all.at[chip], gated_all.at[chip])
    for copy in late:
        copy.wait()
    pack_spread = spread(5, lambda there: pack_send.at[there, plane], pack_recv.at[me, plane])
    settle(out_twins, ow_all, out_pushes)
    for copy in near_pushes + out_pushes:
        copy.wait_recv()
    for k in range(len(order)):
        third[k].wait_recv()

    def flat(buffer):
        held = buffer[...].astype(F32)
        return held.reshape(group, held.shape[2])

    mix = jnp.dot(
        flat(gated_all).astype(BF16),
        ow_all[...].reshape(n * cut, block),
        preferred_element_type=F32,
    )
    mix_all[chip] = mix.astype(BF16)
    fourth = spread(7, lambda there: mix_all.at[chip], mix_all.at[chip])
    drain(2 * len(order))
    forward(pack_spread, pack_recv, pack_twins, pack_pushes)
    settle(pack_twins, pack_recv, pack_pushes)
    for k in range(len(order)):
        table_spread[k].wait_recv()
    for copy in pack_pushes + expert_pushes:
        copy.wait_recv()
    gain = in_line(gain_two)
    gain_rows[...] = gain.reshape(chips, 1, block)

    def take(source):
        span = pl.ds(pl.multiple_of(source * block, block), block)
        held = tok_all[:, :, span].astype(F32).reshape(group, block) + mix_all[source].astype(F32)
        streamed[:, :, span] = held.reshape(chips, rows, block)
        scaled = (held * gain_rows[source]).astype(BF16)
        parts = [
            jnp.dot(scaled, wide[e, i, span, :], preferred_element_type=F32)
            for e in range(2)
            for i in range(2)
        ]
        turned = jnp.concatenate(
            [
                jnp.concatenate([pack_recv[2 * source + j, i, :hidden, :] for i in range(2)], axis=0)
                for j in range(2)
            ],
            axis=1,
        )
        return parts + [across(scaled, turned)], jnp.sum(held * held, axis=1, keepdims=True)

    inner = wide.shape[3]
    spots = [i * inner for i in range(5)]

    def keep(source, fresh):
        parts, squares = take(source)
        for spot, value in zip(spots, parts):
            here = slice(spot, spot + value.shape[1])
            sums_all[:, here] = value if fresh else sums_all[:, here] + value
        return squares

    squares = keep(chip, True)
    lane_at = lax.broadcasted_iota(jnp.int32, (group, rows * n), 1)
    row_at = lax.broadcasted_iota(jnp.int32, (group, rows * n), 0) % rows
    weights_all = jnp.concatenate(
        [jnp.broadcast_to(table[c], (rows, rows * n)) for c in range(chips)], axis=0
    )
    routed = [
        jnp.sum(
            jnp.where(lane_at == row_at * n + 2 * chip + e, weights_all, 0.0),
            axis=1,
            keepdims=True,
        )
        for e in range(2)
    ]
    shared_rows = jnp.concatenate(
        [
            jnp.concatenate([pack_recv[i, j, hidden:, :] for i in range(n)], axis=1)
            for j in range(2)
        ],
        axis=0,
    )
    for k in reversed(range(len(order))):
        fourth[k].wait_recv()
        squares = squares + keep(from_chip(k), False)

    scale = lax.rsqrt(squares / width + epsilon)
    hiddens = []
    for e in range(2):
        gate_sums = sums_all[:, spots[2 * e] : spots[2 * e] + inner] * scale
        up_sums = sums_all[:, spots[2 * e + 1] : spots[2 * e + 1] + inner] * scale
        hiddens.append((jax.nn.silu(gate_sums) * up_sums * routed[e]).astype(BF16))
    both = sums_all[:, spots[4] : spots[4] + 2 * hidden] * scale
    shared_hidden = (jax.nn.silu(both[:, :hidden]) * both[:, hidden:]).astype(BF16)
    half = width // 2
    fifth = []
    for i in range(2):
        span = slice(i * half, (i + 1) * half)
        value = jnp.dot(shared_hidden, shared_rows[:, span], preferred_element_type=F32)
        for e in range(2):
            value = value + jnp.dot(hiddens[e], down[e, :, span], preferred_element_type=F32)
        value = value.reshape(chips, rows, half)
        part[i] = value
        part_send[i] = value.astype(BF16)
        fifth.append(
            spread(
                (8, 9)[i], lambda there: part_send.at[i, there], sum_recv.at[i, chip]
            )
        )
    drain(2 * len(order))
    for i in range(2):
        span = slice(i * half, (i + 1) * half)
        total = streamed[chip, :, span] + part[i, chip]
        for k in reversed(range(len(order))):
            fifth[i][k].wait_recv()
            total = total + sum_recv[i, from_chip(k)].astype(F32)
        mixed_out[:, span] = total.astype(BF16)

    drain()


def flush(*refs):
    sources, targets, sems = refs[:4], refs[4:8], refs[8]
    copies = []
    for i in (1, 2, 0, 3):
        if i == 1:
            for s in range(sources[i].shape[0]):
                copies.append((sources[i].at[s], targets[i].at[s]))
        else:
            copies.append((sources[i], targets[i]))
    started = []
    for i, (source, target) in enumerate(copies):
        copy = pltpu.make_async_copy(source, target, sems.at[i])
        copy.start()
        started.append(copy)
    for copy in started:
        copy.wait()


def fused_shards(n, *args):
    (tokens, first_gain, query_weight, key_weight, value_weight, outgate_weight, igate_weight,
     fgate_weight, igate_bias, fgate_bias, memory_state, norm_state, max_state, head_gain,
     out_weight, second_gain, expert_ids, route_weight, expert_gate, expert_up, expert_down,
     shared_gate, shared_up, shared_down) = args
    rows, width = tokens.shape
    heads, size = memory_state.shape[1], memory_state.shape[3]
    cut = query_weight.shape[1]
    chips = n // 2
    hidden = shared_gate.shape[1] // chips
    inner = expert_gate.shape[2]
    top_count = expert_ids.shape[1]
    lean = shared_down.shape[1]
    operands = (
        tokens, first_gain.reshape(-1, 128), query_weight.T, key_weight.T, value_weight.T,
        outgate_weight.T, igate_weight.T, fgate_weight.T, igate_bias.reshape(1, -1), fgate_bias.reshape(1, -1),
        memory_state, norm_state, max_state, head_gain.reshape(heads, size), out_weight,
        second_gain.reshape(-1, 128), expert_ids, route_weight, expert_gate, expert_up, expert_down,
        shared_gate, shared_up, shared_down.reshape(chips, 2, hidden // 2, lean),
    )
    operands = [pltpu.with_memory_space_constraint(x, pltpu.HBM) for x in operands]
    dma = pltpu.SemaphoreType.DMA
    results = (
        jax.ShapeDtypeStruct((rows, width), BF16),
        jax.ShapeDtypeStruct(memory_state.shape, F32),
        jax.ShapeDtypeStruct(norm_state.shape, F32),
        jax.ShapeDtypeStruct(max_state.shape, F32),
    )
    inside = pl.pallas_call(
        functools.partial(fused, n),
        out_shape=results,
        in_specs=[pl.BlockSpec(memory_space=pltpu.HBM)] * len(operands),
        out_specs=tuple(pl.BlockSpec(memory_space=VMEM) for _ in results),
        scratch_shapes=[
            VMEM((width // 128, 128), BF16),
            VMEM((width // 128, 128), BF16),
            VMEM((2, 1, heads), F32),
            VMEM((2, heads, width), BF16),
            VMEM(norm_state.shape, F32),
            VMEM(max_state.shape, F32),
            VMEM((heads, size), BF16),
            VMEM((rows, top_count), jnp.int32),
            VMEM((rows, top_count), F32),
            VMEM(shared_gate.shape, BF16),
            VMEM(shared_up.shape, BF16),
            VMEM((chips, 2, cut // 2, width // chips), BF16),
            VMEM((4, 2, cut, width), BF16),
            VMEM((2, 2, width, inner), BF16),
            VMEM((2, inner, width), BF16),
            VMEM((chips, rows, width), BF16),
            VMEM((chips, 1, rows * n), F32),
            VMEM((chips * rows, width), F32),
            VMEM((chips, rows, 8 * cut), BF16),
            VMEM((chips, rows, 8 * cut), BF16),
            VMEM((chips, rows, heads * size), BF16),
            VMEM((n, 2, cut // 2, width // chips), BF16),
            VMEM((chips, chips * rows, width // chips), BF16),
            VMEM((chips, rows, width), F32),
            VMEM((chips, 2, 3 * hidden // 2, lean), BF16),
            VMEM((n, 2, 3 * hidden // 2, lean), BF16),
            VMEM((2, chips, rows, width // 2), F32),
            VMEM((2, chips, rows, width // 2), BF16),
            VMEM((2, chips, rows, width // 2), BF16),
            VMEM((chips, 1, width // chips), F32),
            VMEM((chips * rows, 4 * inner + 128), F32),
            dma((24 + 2 * chips,)),
            dma((heads,)),
            dma((10, chips)),
            dma((10, chips)),
            dma((10 + 4 * chips,)),
            dma((10 + 4 * chips,)),
            dma((2 * chips,)),
            dma((2 * chips,)),
        ],
        compiler_params=pltpu.CompilerParams(
            collective_id=0, has_side_effects=True, vmem_limit_bytes=36 * 1024 * 1024
        ),
    )(*operands)
    return pl.pallas_call(
        flush,
        out_shape=results,
        in_specs=[pl.BlockSpec(memory_space=VMEM)] * 4,
        out_specs=tuple(pl.BlockSpec(memory_space=pltpu.HBM) for _ in results),
        scratch_shapes=[dma((rows + 3,))],
        compiler_params=pltpu.CompilerParams(vmem_limit_bytes=1024 * 1024),
    )(*[pltpu.with_memory_space_constraint(x, VMEM) for x in inside])


def fits(n, groups, width, size, heads, cut, hidden_all, experts, rows):
    chips = n // 2
    return (
        n % 4 == 0
        and groups == 2
        and rows * n == 128
        and experts == n
        and heads == chips
        and 2 * cut == size
        and size == 128
        and width % (128 * n) == 0
        and hidden_all % (32 * chips) == 0
        and rows == 8
        and 2 * hidden_all <= 128 * chips
    )


def pick(n, groups, *args):
    tokens, query_weight, memory_state = args[0], args[2], args[10]
    experts, hidden_all = args[18].shape[0] * n, args[21].shape[1]
    if fits(
        n, groups, tokens.shape[1], memory_state.shape[3], memory_state.shape[1], query_weight.shape[1],
        hidden_all, experts, tokens.shape[0],
    ):
        return fused_shards(n, *args)
    return shards(*args)


def solution(mesh):
    placed = (
        P(("grp", "ep"), None),
        P(),
        P(None, "ep"),
        P(None, "ep"),
        P(None, "ep"),
        P(None, "ep"),
        P(),
        P(),
        P(),
        P(),
        P(("grp", "ep"), None, None, None),
        P(("grp", "ep"), None, None),
        P(("grp", "ep"), None),
        P(),
        P("ep", None),
        P(),
        P(("grp", "ep"), None),
        P(("grp", "ep"), None),
        P("ep", None, None),
        P("ep", None, None),
        P("ep", None, None),
        P("ep", None),
        P("ep", None),
        P(None, "ep"),
    )
    return jax.shard_map(
        functools.partial(pick, mesh.shape["ep"], mesh.shape["grp"]),
        mesh=mesh,
        in_specs=placed,
        out_specs=(
            P(("grp", "ep"), None),
            P(("grp", "ep"), None, None, None),
            P(("grp", "ep"), None, None),
            P(("grp", "ep"), None),
        ),
        check_vma=False,
    )
```

```python
import jax
import jax.numpy as jnp
from jax import lax
from jax.experimental import pallas as pl
from jax.experimental.pallas import tpu as pltpu
from jax.sharding import PartitionSpec as P
import functools

epsilon = 1e-06


def rms_scale(values, gain):
    return (
        values
        * lax.rsqrt(jnp.mean(values * values, axis=-1, keepdims=True) + epsilon)
        * gain.astype(jnp.float32)
    )


def cell_step(
    normed,
    query,
    key_proj,
    value_proj,
    outgate,
    igate_weight,
    fgate_weight,
    igate_bias,
    fgate_bias,
    memory_state,
    norm_state,
    max_state,
    head_gain,
):
    row_count, head_count = max_state.shape
    head_size = memory_state.shape[-1]
    input_gate = jnp.dot(normed, igate_weight, preferred_element_type=jnp.float32) + igate_bias
    forget_log = jax.nn.log_sigmoid(
        jnp.dot(normed, fgate_weight, preferred_element_type=jnp.float32) + fgate_bias
    )
    query_heads = query.astype(jnp.float32).reshape(row_count, head_count, head_size)
    key_heads = key_proj.astype(jnp.float32).reshape(
        row_count, head_count, head_size
    ) * head_size ** (-0.5)
    value_heads = value_proj.astype(jnp.float32).reshape(row_count, head_count, head_size)
    max_next = jnp.maximum(forget_log + max_state, input_gate)
    decay_rate = jnp.exp(forget_log + max_state - max_next)
    injected = jnp.exp(input_gate - max_next)
    memory_next = decay_rate[:, :, None, None] * memory_state + injected[:, :, None, None] * (
        key_heads[:, :, :, None] * value_heads[:, :, None, :]
    )
    norm_next = decay_rate[:, :, None] * norm_state + injected[:, :, None] * key_heads
    numerator = jnp.einsum(
        "shd,shde->she", query_heads, memory_next, precision=lax.Precision.HIGHEST
    )
    denominator = jnp.maximum(
        jnp.abs(jnp.sum(query_heads * norm_next, axis=-1)), jnp.exp(-max_next)
    )
    readout = numerator / denominator[:, :, None]
    readout = rms_scale(readout, head_gain.reshape(head_count, head_size))
    gated = readout.reshape(row_count, head_count * head_size) * jax.nn.sigmoid(
        outgate.astype(jnp.float32)
    )
    return (gated.astype(jnp.bfloat16), memory_next, norm_next, max_next)


def shards(
    tokens,
    first_gain,
    query_weight,
    key_weight,
    value_weight,
    outgate_weight,
    igate_weight,
    fgate_weight,
    igate_bias,
    fgate_bias,
    memory_state,
    norm_state,
    max_state,
    head_gain,
    out_weight,
    second_gain,
    expert_ids,
    route_weight,
    expert_gate,
    expert_up,
    expert_down,
    shared_gate,
    shared_up,
    shared_down,
):
    own_rows = tokens.shape[0]
    devices = lax.axis_size("ep")
    top_count = expert_ids.shape[1]
    capacity = max(2, 2 * own_rows * top_count // devices)
    inputs = tokens.astype(jnp.float32)
    normed = rms_scale(inputs, first_gain).astype(jnp.bfloat16)
    block_rows = lax.all_gather(normed, "ep", axis=0, tiled=True)
    columns = jnp.stack(
        [
            jnp.dot(block_rows, matrix, preferred_element_type=jnp.float32).astype(jnp.bfloat16)
            for matrix in (query_weight, key_weight, value_weight, outgate_weight)
        ]
    )
    projected = lax.all_to_all(columns, "ep", split_axis=1, concat_axis=2, tiled=True)
    gated, memory_next, norm_next, max_next = cell_step(
        normed,
        projected[0],
        projected[1],
        projected[2],
        projected[3],
        igate_weight,
        fgate_weight,
        igate_bias,
        fgate_bias,
        memory_state,
        norm_state,
        max_state,
        head_gain,
    )
    picked = gated
    mix_sums = jnp.dot(
        picked,
        lax.all_gather(out_weight, "ep", axis=0, tiled=True),
        preferred_element_type=jnp.float32,
    )
    stream = inputs + mix_sums.astype(jnp.bfloat16).astype(jnp.float32)
    normed_two = rms_scale(stream, second_gain).astype(jnp.bfloat16)
    block_rows = (
        lax.all_gather(shared_gate, "ep", axis=0, tiled=True),
        lax.all_gather(shared_up, "ep", axis=0, tiled=True),
    )
    picked = normed_two
    gate_shared = jnp.dot(picked, block_rows[0], preferred_element_type=jnp.float32)
    up_shared = jnp.dot(picked, block_rows[1], preferred_element_type=jnp.float32)
    hidden_shared = (jax.nn.silu(gate_shared) * up_shared).astype(jnp.bfloat16)
    shared_result = jnp.dot(
        hidden_shared,
        lax.all_gather(shared_down, "ep", axis=1, tiled=True),
        preferred_element_type=jnp.float32,
    )
    choose = (expert_ids[:, :, None] == jnp.arange(devices, dtype=jnp.int32)[None, None, :]).astype(
        jnp.int32
    )
    counted = jnp.sum(choose, axis=1)
    ranking = jnp.cumsum(counted, axis=0) - counted
    slot_index = jnp.sum(choose * ranking[:, None, :], axis=2)
    slot_ids = jnp.arange(capacity, dtype=jnp.int32)
    selector = counted.T[:, None, :] * (ranking.T[:, None, :] == slot_ids[None, :, None]).astype(
        jnp.int32
    )
    outgoing = jnp.einsum(
        "ecr,rd->ecd", selector.astype(jnp.bfloat16), normed_two, preferred_element_type=jnp.float32
    ).astype(jnp.bfloat16)
    arrived = lax.all_to_all(outgoing, "ep", split_axis=0, concat_axis=0, tiled=True)
    sources, slots, width = arrived.shape
    flat_rows = arrived.reshape(sources * slots, width)
    gate_sums = jnp.dot(flat_rows, expert_gate[0], preferred_element_type=jnp.float32)
    up_sums = jnp.dot(flat_rows, expert_up[0], preferred_element_type=jnp.float32)
    hidden = (jax.nn.silu(gate_sums) * up_sums).astype(jnp.bfloat16)
    result = jnp.dot(hidden, expert_down[0], preferred_element_type=jnp.float32).astype(
        jnp.bfloat16
    )
    results = lax.all_to_all(
        result.reshape(sources, slots, width), "ep", split_axis=0, concat_axis=0, tiled=True
    )
    flat_results = results.reshape(devices * capacity, results.shape[2])
    picked_results = flat_results[expert_ids * capacity + slot_index]
    routed = jnp.sum(route_weight[:, :, None] * picked_results.astype(jnp.float32), axis=1)
    mixed_out = (stream + routed + shared_result).astype(jnp.bfloat16)
    return (mixed_out, memory_next, norm_next, max_next)


ANY, VMEM = pl.ANY, pltpu.VMEM
F32, BF16 = jnp.float32, jnp.bfloat16


def across(left, right):
    return lax.dot_general(left, right, (((1,), (1,)), ((), ())), preferred_element_type=F32)


def turned_dot(left, right):
    return lax.dot_general(
        left.astype(BF16),
        right.astype(BF16),
        (((0,), (0,)), ((), ())),
        preferred_element_type=F32,
    )


def in_line(gain):
    held = gain[...].astype(F32)
    return jnp.concatenate([held[i : i + 1] for i in range(held.shape[0])], axis=1)


def offsets(chips):
    ring = chips // 2
    steps = [(step, flip) for step in range(ring) for flip in (1, 0) if step or flip]
    return sorted(steps, key=lambda o: -(min(o[0], ring - o[0]) + o[1]))


def fused(n, *refs):
    (tokens, first_gain, query_weight, key_weight, value_weight, outgate_weight, igate_weight,
     fgate_weight, igate_bias, fgate_bias, memory_state, norm_state, max_state, head_gain,
     out_weight, second_gain, expert_ids, route_weight, expert_gate, expert_up, expert_down,
     shared_gate, shared_up, shared_down,
     mixed_out, memory_next, norm_next, max_next,
     gain_one, gain_two, bias, gates_in, norm_in, max_in, gain_head, ids, route, sgate, sup,
     out_own, proj, wide, down, tok_all, table, normed, column_send, column_recv, gated_all,
     ow_all, mix_all, streamed, pack_send, pack_recv, part, part_send, sum_recv, gain_rows, sums_all,
     local_sem, memory_sem, send_sem, recv_sem, pair_send, pair_recv, twin_send, twin_recv) = refs
    rows, width = tokens.shape
    heads, size = memory_state.shape[1], memory_state.shape[3]
    cut = query_weight.shape[0]
    chips = n // 2
    hidden = sgate.shape[1] // chips
    block = width // chips
    group = chips * rows
    top_count = expert_ids.shape[1]
    ring = chips // 2
    me = lax.axis_index("ep")
    plane = lax.axis_index("grp")
    other = 1 - plane
    side, chip = me % 2, me // 2
    partner = me + 1 - 2 * side
    order = offsets(chips)

    def to_chip(k):
        step, flip = order[k]
        return 2 * ((chip // 2 + step) % ring) + (chip + flip) % 2

    def from_chip(k):
        step, flip = order[k]
        return 2 * ((chip // 2 + ring - step) % ring) + (chip + flip) % 2

    barrier = pltpu.get_barrier_semaphore()
    for k in range(len(order)):
        pl.semaphore_signal(
            barrier,
            inc=1,
            device_id={"ep": 2 * to_chip(k) + side},
            device_id_type=pl.DeviceIdType.MESH,
        )
    pl.semaphore_signal(
        barrier, inc=1, device_id={"ep": partner}, device_id_type=pl.DeviceIdType.MESH
    )

    pl.semaphore_signal(
        barrier, inc=1, device_id={"grp": other}, device_id_type=pl.DeviceIdType.MESH
    )
    loads = []

    def load(source, target):
        copy = pltpu.make_async_copy(source, target, local_sem.at[len(loads)])
        copy.start()
        loads.append(copy)
        return copy

    token_load = load(tokens, tok_all.at[chip])
    gain_load = load(first_gain, gain_one)
    early = [
        load(igate_weight, gates_in.at[0]),
        load(fgate_weight, gates_in.at[1]),
        load(igate_bias, bias.at[0]),
        load(fgate_bias, bias.at[1]),
        load(max_state, max_in),
        load(expert_ids, ids),
        load(route_weight, route),
        load(shared_gate, sgate),
        load(shared_up, sup),
        load(shared_down.at[:, 0], pack_send.at[:, 0, hidden:]),
        load(shared_down.at[:, 1], pack_send.at[:, 1, hidden:]),
        load(norm_state, norm_in),
        load(head_gain, gain_head),
        load(second_gain, gain_two),
    ]
    weights = (query_weight, key_weight, value_weight, outgate_weight)
    proj_loads = [load(matrix, proj.at[i, side]) for i, matrix in enumerate(weights)]
    out_load = load(out_weight, out_own)
    memory_loads = []
    for i in range(4):
        some = pl.ds(i * rows // 4, rows // 4)
        memory_loads.append(
            pltpu.make_async_copy(memory_state.at[some], memory_next.at[some], memory_sem.at[i])
        )
        memory_loads[i].start()
    late = [
        load(expert_gate.at[0], wide.at[side, 0]),
        load(expert_up.at[0], wide.at[side, 1]),
        load(expert_down.at[0], down.at[side]),
    ]
    token_load.wait()
    unsent = []

    def spread(which, source, target):
        copies = []
        for k in range(len(order)):
            there = to_chip(k)
            copy = pltpu.make_async_remote_copy(
                src_ref=source(there),
                dst_ref=target,
                send_sem=send_sem.at[which, k],
                recv_sem=recv_sem.at[which, k],
                device_id={"ep": 2 * there + side},
                device_id_type=pl.DeviceIdType.MESH,
            )
            copy.start()
            copies.append(copy)
        unsent.extend(copies)
        return copies

    twins = []

    def cross(source, target):
        copy = pltpu.make_async_remote_copy(
            src_ref=source,
            dst_ref=target,
            send_sem=twin_send.at[len(twins)],
            recv_sem=twin_recv.at[len(twins)],
            device_id={"grp": other},
            device_id_type=pl.DeviceIdType.MESH,
        )
        copy.start()
        twins.append(copy)
        return copy

    pairs = []

    def push(source, target):
        copy = pltpu.make_async_remote_copy(
            src_ref=source,
            dst_ref=target,
            send_sem=pair_send.at[len(pairs)],
            recv_sem=pair_recv.at[len(pairs)],
            device_id={"ep": partner},
            device_id_type=pl.DeviceIdType.MESH,
        )
        copy.start()
        pairs.append(copy)
        return copy

    drained = [0, 0, 0]

    def drain(keep=0):
        for i, held in enumerate((unsent, pairs, twins)):
            stop = len(held) - (keep if i == 0 else 0)
            for copy in held[drained[i] : stop] if i == 0 or not keep else []:
                copy.wait_send()
                drained[i] += 1

    pl.semaphore_wait(barrier, len(order) + 2)
    first = spread(0, lambda there: tok_all.at[chip], tok_all.at[chip])
    proj_pushes = [push(matrix, proj.at[i, side]) for i, matrix in enumerate(weights)]

    expert_pushes = [
        push(expert_gate.at[0], wide.at[side, 0]),
        push(expert_up.at[0], wide.at[side, 1]),
        push(expert_down.at[0], down.at[side]),
    ]
    gain_load.wait()
    gain = in_line(gain_one)

    def norm_rows(source):
        values = rms_scale(tok_all[source].astype(F32), gain)
        normed[pl.ds(pl.multiple_of(source * rows, rows), rows), :] = values
        return values.astype(BF16)

    own = norm_rows(chip)
    for copy in early:
        copy.wait()
    lanes = lax.broadcasted_iota(jnp.int32, (rows, rows * n), 1)
    mine = lanes // n == lax.broadcasted_iota(jnp.int32, (rows, rows * n), 0)
    routes = jnp.zeros((rows, rows * n), F32)
    for t in range(top_count):
        routes = routes + jnp.where(
            mine & (lanes % n == ids[:, t : t + 1]), route[:, t : t + 1], 0.0
        )
    table[chip] = jnp.sum(routes, axis=0, keepdims=True)
    for i, matrix in enumerate((sgate, sup)):
        turned = matrix[...].astype(F32).T.reshape(chips, hidden, matrix.shape[0])
        pack_send[:, i, :hidden, :] = turned.astype(BF16)
    input_gate = across(own, gates_in[0]) + bias[0]
    forget_log = jax.nn.log_sigmoid(across(own, gates_in[1]) + bias[1])
    kept = forget_log + max_in[...]
    top = jnp.maximum(kept, input_gate)
    max_next[...] = top
    decay_rate = jnp.exp(kept - top)
    injected = jnp.exp(input_gate - top)
    floor = jnp.exp(-top)
    for copy in proj_loads:
        copy.wait()
    for copy in proj_pushes:
        copy.wait_recv()

    for k in reversed(range(len(order))):
        first[k].wait_recv()
        norm_rows(from_chip(k))

    columns = across(normed[...].astype(BF16), proj[...].reshape(8 * cut, width))
    column_send[...] = columns.reshape(chips, rows, 8 * cut).astype(BF16)
    second = spread(1, lambda there: column_send.at[there], column_recv.at[chip])
    column_recv[chip] = column_send[chip]
    out_load.wait()

    def out_columns(there):
        rows_here = pl.ds(pl.multiple_of(plane * (cut // 2), cut // 2), cut // 2)
        return out_own.at[rows_here, pl.ds(pl.multiple_of(there * block, block), block)]

    out_spread = spread(2, out_columns, ow_all.at[chip, side, plane])
    table_spread = spread(3, lambda there: table.at[chip], table.at[chip])
    ow_all[chip, side, plane] = out_columns(chip)[...]
    pack_recv[chip, side, plane] = pack_send[chip, plane]
    out_pushes, pack_pushes, out_twins, pack_twins = [], [], [], []

    def forward(copies, buffer, crossed, pushed):
        for copy in copies:
            copy.wait_recv()
        held = buffer.at[:, side, plane]
        crossed.append(cross(held, held))
        pushed.append(push(held, held))

    def settle(crossed, buffer, pushed):
        for copy in crossed:
            copy.wait_recv()
        held = buffer.at[:, side, other]
        pushed.append(push(held, held))

    for copy in memory_loads:
        copy.wait()
    for k in range(len(order)):
        second[k].wait_recv()

    place = lax.broadcasted_iota(jnp.int32, (rows, rows * size), 1) // size
    diagonal = place == lax.broadcasted_iota(jnp.int32, (rows, rows * size), 0)
    for h in range(heads):
        piece = column_recv[h].astype(F32)
        query, keyed, valued, outgate = [piece[:, i * size : (i + 1) * size] for i in range(4)]
        scale = injected[:, h : h + 1] * size ** (-0.5)
        decay = jnp.broadcast_to(decay_rate[:, h : h + 1], (rows, size))
        norm = decay * norm_in[:, h, :] + scale * keyed
        norm_next[:, h, :] = norm
        bottom = jnp.maximum(
            jnp.abs(jnp.sum(query * norm, axis=-1, keepdims=True)), floor[:, h : h + 1]
        )
        spread_value = jnp.where(diagonal, jnp.concatenate([scale * valued] * rows, axis=1), 0.0)
        high = spread_value.astype(BF16).astype(F32)
        outer = turned_dot(
            jnp.concatenate([keyed, keyed], axis=0),
            jnp.concatenate([high, spread_value - high], axis=0),
        )
        query_columns = query.T
        tops = []
        for s in range(rows):
            cell = (
                decay[s : s + 1, :] * memory_next[s, h] + outer[:, s * size : (s + 1) * size]
            )
            memory_next[s, h] = cell
            tops.append(jnp.sum(query_columns[:, s : s + 1] * cell, axis=0, keepdims=True))
        readout = jnp.concatenate(tops, axis=0) / bottom
        readout = rms_scale(readout, gain_head[h : h + 1, :])
        gated_all[chip, :, h * size : (h + 1) * size] = (
            readout * jax.nn.sigmoid(outgate)
        ).astype(BF16)
        if h == heads // 2:
            forward(out_spread, ow_all, out_twins, out_pushes)

    drain(len(unsent) - len(order))
    third = spread(0, lambda there: gated_all.at[chip], gated_all.at[chip])
    for copy in late:
        copy.wait()
    pack_spread = spread(4, lambda there: pack_send.at[there, plane], pack_recv.at[chip, side, plane])
    settle(out_twins, ow_all, out_pushes)
    for copy in out_pushes:
        copy.wait_recv()
    for k in range(len(order)):
        third[k].wait_recv()

    def flat(buffer):
        held = buffer[...].astype(F32)
        return held.reshape(group, held.shape[2])

    mix = jnp.dot(
        flat(gated_all).astype(BF16),
        ow_all[...].reshape(n * cut, block),
        preferred_element_type=F32,
    )
    mix_all[chip] = mix.astype(BF16)
    drain(len(unsent) - 2 * len(order))
    fourth = spread(1, lambda there: mix_all.at[chip], mix_all.at[chip])
    drain(2 * len(order))
    forward(pack_spread, pack_recv, pack_twins, pack_pushes)
    settle(pack_twins, pack_recv, pack_pushes)
    for k in range(len(order)):
        table_spread[k].wait_recv()
    for copy in pack_pushes + expert_pushes:
        copy.wait_recv()
    gain = in_line(gain_two)
    gain_rows[...] = gain.reshape(chips, 1, block)

    def take(source):
        span = pl.ds(pl.multiple_of(source * block, block), block)
        held = tok_all[:, :, span].astype(F32).reshape(group, block) + mix_all[source].astype(F32)
        streamed[:, :, span] = held.reshape(chips, rows, block)
        scaled = (held * gain_rows[source]).astype(BF16)
        parts = [
            jnp.dot(scaled, wide[e, i, span, :], preferred_element_type=F32)
            for e in range(2)
            for i in range(2)
        ]
        turned = jnp.concatenate(
            [
                jnp.concatenate([pack_recv[source, j, i, :hidden, :] for i in range(2)], axis=0)
                for j in range(2)
            ],
            axis=1,
        )
        return parts + [across(scaled, turned)], jnp.sum(held * held, axis=1, keepdims=True)

    inner = wide.shape[3]
    spots = [i * inner for i in range(5)]

    def keep(source, fresh):
        parts, squares = take(source)
        for spot, value in zip(spots, parts):
            here = slice(spot, spot + value.shape[1])
            sums_all[:, here] = value if fresh else sums_all[:, here] + value
        return squares

    squares = keep(chip, True)
    lane_at = lax.broadcasted_iota(jnp.int32, (group, rows * n), 1)
    row_at = lax.broadcasted_iota(jnp.int32, (group, rows * n), 0) % rows
    weights_all = jnp.concatenate(
        [jnp.broadcast_to(table[c], (rows, rows * n)) for c in range(chips)], axis=0
    )
    routed = [
        jnp.sum(
            jnp.where(lane_at == row_at * n + 2 * chip + e, weights_all, 0.0),
            axis=1,
            keepdims=True,
        )
        for e in range(2)
    ]
    shared_rows = jnp.concatenate(
        [
            jnp.concatenate([pack_recv[i // 2, i % 2, j, hidden:, :] for i in range(n)], axis=1)
            for j in range(2)
        ],
        axis=0,
    )
    for k in reversed(range(len(order))):
        fourth[k].wait_recv()
        squares = squares + keep(from_chip(k), False)

    scale = lax.rsqrt(squares / width + epsilon)
    hiddens = []
    for e in range(2):
        gate_sums = sums_all[:, spots[2 * e] : spots[2 * e] + inner] * scale
        up_sums = sums_all[:, spots[2 * e + 1] : spots[2 * e + 1] + inner] * scale
        hiddens.append((jax.nn.silu(gate_sums) * up_sums * routed[e]).astype(BF16))
    both = sums_all[:, spots[4] : spots[4] + 2 * hidden] * scale
    shared_hidden = (jax.nn.silu(both[:, :hidden]) * both[:, hidden:]).astype(BF16)
    half = width // 2
    fifth = []
    for i in range(2):
        span = slice(i * half, (i + 1) * half)
        value = jnp.dot(shared_hidden, shared_rows[:, span], preferred_element_type=F32)
        for e in range(2):
            value = value + jnp.dot(hiddens[e], down[e, :, span], preferred_element_type=F32)
        value = value.reshape(chips, rows, half)
        part[i] = value
        part_send[i] = value.astype(BF16)
        fifth.append(
            spread(
                (0, 2)[i], lambda there: part_send.at[i, there], sum_recv.at[i, chip]
            )
        )
    drain(2 * len(order))
    for i in range(2):
        span = slice(i * half, (i + 1) * half)
        total = streamed[chip, :, span] + part[i, chip]
        for k in reversed(range(len(order))):
            fifth[i][k].wait_recv()
            total = total + sum_recv[i, from_chip(k)].astype(F32)
        mixed_out[:, span] = total.astype(BF16)

    drain()


def flush(*refs):
    sources, targets, sems = refs[:4], refs[4:8], refs[8]
    copies = []
    for i in (1, 2, 0, 3):
        if i == 1:
            for s in range(sources[i].shape[0]):
                copies.append((sources[i].at[s], targets[i].at[s]))
        else:
            copies.append((sources[i], targets[i]))
    started = []
    for i, (source, target) in enumerate(copies):
        copy = pltpu.make_async_copy(source, target, sems.at[i])
        copy.start()
        started.append(copy)
    for copy in started:
        copy.wait()


def fused_shards(n, *args):
    (tokens, first_gain, query_weight, key_weight, value_weight, outgate_weight, igate_weight,
     fgate_weight, igate_bias, fgate_bias, memory_state, norm_state, max_state, head_gain,
     out_weight, second_gain, expert_ids, route_weight, expert_gate, expert_up, expert_down,
     shared_gate, shared_up, shared_down) = args
    rows, width = tokens.shape
    heads, size = memory_state.shape[1], memory_state.shape[3]
    cut = query_weight.shape[1]
    chips = n // 2
    hidden = shared_gate.shape[1] // chips
    inner = expert_gate.shape[2]
    top_count = expert_ids.shape[1]
    lean = shared_down.shape[1]
    operands = (
        tokens, first_gain.reshape(-1, 128), query_weight.T, key_weight.T, value_weight.T,
        outgate_weight.T, igate_weight.T, fgate_weight.T, igate_bias.reshape(1, -1), fgate_bias.reshape(1, -1),
        memory_state, norm_state, max_state, head_gain.reshape(heads, size), out_weight,
        second_gain.reshape(-1, 128), expert_ids, route_weight, expert_gate, expert_up, expert_down,
        shared_gate, shared_up, shared_down.reshape(chips, 2, hidden // 2, lean),
    )
    operands = [pltpu.with_memory_space_constraint(x, pltpu.HBM) for x in operands]
    dma = pltpu.SemaphoreType.DMA
    results = (
        jax.ShapeDtypeStruct((rows, width), BF16),
        jax.ShapeDtypeStruct(memory_state.shape, F32),
        jax.ShapeDtypeStruct(norm_state.shape, F32),
        jax.ShapeDtypeStruct(max_state.shape, F32),
    )
    inside = pl.pallas_call(
        functools.partial(fused, n),
        out_shape=results,
        in_specs=[pl.BlockSpec(memory_space=pltpu.HBM)] * len(operands),
        out_specs=tuple(pl.BlockSpec(memory_space=VMEM) for _ in results),
        scratch_shapes=[
            VMEM((width // 128, 128), BF16),
            VMEM((width // 128, 128), BF16),
            VMEM((2, 1, heads), F32),
            VMEM((2, heads, width), BF16),
            VMEM(norm_state.shape, F32),
            VMEM(max_state.shape, F32),
            VMEM((heads, size), BF16),
            VMEM((rows, top_count), jnp.int32),
            VMEM((rows, top_count), F32),
            VMEM(shared_gate.shape, BF16),
            VMEM(shared_up.shape, BF16),
            VMEM(out_weight.shape, BF16),
            VMEM((4, 2, cut, width), BF16),
            VMEM((2, 2, width, inner), BF16),
            VMEM((2, inner, width), BF16),
            VMEM((chips, rows, width), BF16),
            VMEM((chips, 1, rows * n), F32),
            VMEM((chips * rows, width), F32),
            VMEM((chips, rows, 8 * cut), BF16),
            VMEM((chips, rows, 8 * cut), BF16),
            VMEM((chips, rows, heads * size), BF16),
            VMEM((chips, 2, 2, cut // 2, width // chips), BF16),
            VMEM((chips, chips * rows, width // chips), BF16),
            VMEM((chips, rows, width), F32),
            VMEM((chips, 2, 3 * hidden // 2, lean), BF16),
            VMEM((chips, 2, 2, 3 * hidden // 2, lean), BF16),
            VMEM((2, chips, rows, width // 2), F32),
            VMEM((2, chips, rows, width // 2), BF16),
            VMEM((2, chips, rows, width // 2), BF16),
            VMEM((chips, 1, width // chips), F32),
            VMEM((chips * rows, 4 * inner + 128), F32),
            dma((24,)),
            dma((4,)),
            dma((5, chips - 1)),
            dma((5, chips - 1)),
            dma((11,)),
            dma((11,)),
            dma((2,)),
            dma((2,)),
        ],
        compiler_params=pltpu.CompilerParams(
            collective_id=0, has_side_effects=True, vmem_limit_bytes=36 * 1024 * 1024
        ),
    )(*operands)
    return pl.pallas_call(
        flush,
        out_shape=results,
        in_specs=[pl.BlockSpec(memory_space=VMEM)] * 4,
        out_specs=tuple(pl.BlockSpec(memory_space=pltpu.HBM) for _ in results),
        scratch_shapes=[dma((rows + 3,))],
        compiler_params=pltpu.CompilerParams(vmem_limit_bytes=1024 * 1024),
    )(*[pltpu.with_memory_space_constraint(x, VMEM) for x in inside])


def fits(n, groups, width, size, heads, cut, hidden_all, experts, rows):
    chips = n // 2
    return (
        n % 4 == 0
        and groups == 2
        and rows * n == 128
        and experts == n
        and heads == chips
        and 2 * cut == size
        and size == 128
        and width % (128 * n) == 0
        and hidden_all % (32 * chips) == 0
        and rows == 8
        and 2 * hidden_all <= 128 * chips
    )


def pick(n, groups, *args):
    tokens, query_weight, memory_state = args[0], args[2], args[10]
    experts, hidden_all = args[18].shape[0] * n, args[21].shape[1]
    if fits(
        n, groups, tokens.shape[1], memory_state.shape[3], memory_state.shape[1], query_weight.shape[1],
        hidden_all, experts, tokens.shape[0],
    ):
        return fused_shards(n, *args)
    return shards(*args)


def solution(mesh):
    placed = (
        P(("grp", "ep"), None),
        P(),
        P(None, "ep"),
        P(None, "ep"),
        P(None, "ep"),
        P(None, "ep"),
        P(),
        P(),
        P(),
        P(),
        P(("grp", "ep"), None, None, None),
        P(("grp", "ep"), None, None),
        P(("grp", "ep"), None),
        P(),
        P("ep", None),
        P(),
        P(("grp", "ep"), None),
        P(("grp", "ep"), None),
        P("ep", None, None),
        P("ep", None, None),
        P("ep", None, None),
        P("ep", None),
        P("ep", None),
        P(None, "ep"),
    )
    return jax.shard_map(
        functools.partial(pick, mesh.shape["ep"], mesh.shape["grp"]),
        mesh=mesh,
        in_specs=placed,
        out_specs=(
            P(("grp", "ep"), None),
            P(("grp", "ep"), None, None, None),
            P(("grp", "ep"), None, None),
            P(("grp", "ep"), None),
        ),
        check_vma=False,
    )
```
